512 devices in a mesh: sp: 32 (over z, core), tp: 16 (over y, x).
Axes of the slice: x: 4, y: 4, z: 16, core: 2. Of those that a mesh axis runs over, the one named last changes fastest.
Arguments:
- stream: bfloat16 [12288, 2048], P('sp'), may hold values from -6 to 6
- inner_act: bfloat16 [12288, 4096], P('sp', 'tp'), may hold values from -6 to 6
- gate_act: bfloat16 [12288, 4096], P('sp', 'tp'), may hold values from -6 to 6
- state_write: bfloat16 [12288, 16, 128], P('sp', 'tp'), may hold values from -6 to 6
- state_read: bfloat16 [12288, 16, 128], P('sp', 'tp'), may hold values from -6 to 6
- step_raw: bfloat16 [12288, 64], P('sp', 'tp'), may hold values from -4.6 to 4.1
- conv_inner: bfloat16 [4, 4096], P(None, 'tp'), may hold values from -3 to 3
- conv_write: bfloat16 [4, 16, 128], P(None, 'tp'), may hold values from -3 to 3
- conv_read: bfloat16 [4, 16, 128], P(None, 'tp'), may hold values from -3 to 3
- step_bias: float32 [64], P('tp'), may hold values from -0.5 to 0.5
- decay_log: float32 [64], P('tp'), may hold values from -13 to -2.52, as said below
- inner_gain: float32 [4096], P('tp'), may hold values from 0.1 to 1.9
- out_weight: bfloat16 [4096, 2048], P('tp'), may hold values from -0.09375 to 0.09375
- ffn_gain: float32 [2048], replicated, may hold values from 0.1 to 1.9
- expert_ids: int32 [12288, 2], P('sp'), may hold values from 0 to 31, all different within a row; in each aligned block of 384 rows (0 to 383, 384 to 767, ...) at most 48 rows name the same one
- expert_weights: float32 [12288, 2], P('sp'), may hold values from 0.1 to 1
- expert_gate: bfloat16 [32, 2048, 1024], P('sp', None, 'tp'), may hold values from -0.125 to 0.125
- expert_up: bfloat16 [32, 2048, 1024], P('sp', None, 'tp'), may hold values from -0.125 to 0.125
- expert_down: bfloat16 [32, 1024, 2048], P('sp', None, 'tp'), may hold values from -0.1875 to 0.1875
Outputs:
- layer_out: bfloat16 [12288, 2048], P('sp', 'tp')
The draws below stay inside these ranges and needn't reach their ends.
Inputs may be any that keep to these rules, and one draw needn't show every extreme that they name: The logarithm of a per-position decay rate: exp(decay_log) lies between 0.1 / 12288 and 0.08. `expert_ids`: each row names 2 different experts. Among the rows of one index of sp (384 tokens) no expert is named more than 48 times, a bound that some block reaches there.
All inputs are finite; a program needn't handle non-finite values.
Results may differ from the reference program's by a relative error of at most 0.014.
Values may be sent and summed in bfloat16 or wider, within the bound.
A program may use at most 64 MiB of HBM per device.

```python
import math
import jax
import jax.numpy as jnp
import numpy as np
from jax import lax

D = 2048
HEADS = 64
HEADDIM = 64
GROUPS = 16
STATE = 128
CONV = 4
BLOCK = 64
FF = 1024
EXPERTS = 32
TOPK = 2
TOK_SP = 384
D_INNER = 4096
TOKENS = 12288
CAP = 48
N_SP = 32
N_TP = 16


def draw_step_raw(key, part):
    key_noise, key_device, key_block = jax.random.split(jax.random.fold_in(key, 11), 3)
    jitter = 0.7 * jax.random.truncated_normal(key_noise, -3.0, 3.0, (TOKENS, HEADS), jnp.float32)
    device_shift = jax.random.uniform(key_device, (TOKENS // TOK_SP, 1, HEADS), jnp.float32, -2.0, 1.5)
    block_shift = jax.random.uniform(key_block, (TOKENS // BLOCK, 1, HEADS), jnp.float32, -0.5, 0.5)
    shifted = jitter.reshape(TOKENS // TOK_SP, TOK_SP, HEADS) + device_shift
    shifted = shifted.reshape(TOKENS // BLOCK, BLOCK, HEADS) + block_shift
    return shifted.reshape(TOKENS, HEADS).astype(jnp.bfloat16)


def draw_decay_log(key, part):
    key_pick, key_level = jax.random.split(jax.random.fold_in(key, 23))
    slow_share = 0.5
    slower = jax.random.bernoulli(key_pick, slow_share, (HEADS,))
    level = jax.random.uniform(key_level, (HEADS,), jnp.float32)
    slow_log = math.log(0.1) + level * math.log(5.0) - math.log(TOKENS)
    fast_log = math.log(0.02) + level * math.log(4.0)
    return jnp.where(slower, slow_log, fast_log).astype(jnp.float32)


def level_of(key, extent, cuts, smallest, high):
    gain, own = 1.0, jax.random.fold_in(key, 6)
    for dim, shards_of in cuts:
        steps = jnp.exp(jax.random.uniform(jax.random.fold_in(own, dim), (shards_of,), jnp.float32, smallest / len(cuts), high / len(cuts)))
        gain = gain * jnp.repeat(steps, extent[dim] // shards_of).reshape([-1 if axis == dim else 1 for axis in range(len(extent))])
    return gain


def routed_block(rng, own, number, rows, count, top, bound, skew):
    order = jax.random.permutation(rng, count)
    packed, ordinary = shares(count, rows * top, bound, skew, True), shares(count, rows * top, bound, skew, False)
    places = jnp.arange(count)

    def named(tallies, rotation):
        used = int((tallies > 0).sum())
        fixed = max(1, used // 4)
        passed = fixed + (places - fixed + rotation * (used - fixed)) % max(1, count - fixed)
        return jnp.zeros((count,), jnp.int32).at[order[jnp.where(places < fixed, places, passed)]].set(jnp.asarray(tallies, jnp.int32))

    tallies = jnp.where(number % 4 == 0, named(packed, number // 4), named(ordinary, number - number // 4 - 1))
    mixed = jax.random.permutation(jax.random.fold_in(own, 3), count)
    donor, receiver = mixed[0:count // 2 * 2:2], mixed[1:count // 2 * 2:2]
    room = jnp.minimum(tallies[donor] - 1, bound - tallies[receiver]) // 2
    room = jnp.where((donor == order[0]) | (receiver == order[0]) | (tallies[receiver] == 0), 0, jnp.maximum(room, 0))
    passed = jax.random.randint(jax.random.fold_in(own, 4), (count // 2,), 0, 1 << 20) % (room + 1)
    tallies = tallies.at[donor].add(-passed).at[receiver].add(passed)
    members = jnp.searchsorted(jnp.cumsum(tallies), jnp.arange(rows * top), side="right").astype(jnp.int32)
    listing = members.reshape(top, rows).T
    listing = listing[jax.random.permutation(jax.random.fold_in(own, 1), rows)]
    rotation = jax.random.randint(jax.random.fold_in(own, 2), (rows, 1), 0, top)
    return jnp.take_along_axis(listing, (jnp.arange(top)[None, :] + rotation) % top, axis=1)


def shares(count, total, bound, slope, full):
    weights = [(1 << 20) // math.isqrt(standing ** slope) + 1 for standing in range(1, count + 1)]
    largest = bound if full else min(bound, max(-(-total // count), total * weights[0] // sum(weights)))
    least = 1 if total - largest >= count - 1 else 0
    holding, rest = [largest] + [least] * (count - 1), total - largest - least * (count - 1)
    while rest > 0:
        candidates = [i for i in range(1, count) if holding[i] < largest] or [i for i in range(1, count) if holding[i] < bound]
        whole, budget = sum([weights[i] for i in candidates]), rest
        for i in candidates:
            extra = min(bound - holding[i], max(1, budget * weights[i] // whole), rest)
            holding[i] = holding[i] + extra
            rest = rest - extra
    return np.array(holding)


def centred(stream_key, shape, scale, limit, shards=(), held_as=jnp.bfloat16):
    loudness = level_of(stream_key, shape, shards, -0.22, 0.18) if shards else 1.0
    result = jax.random.normal(stream_key, shape, jnp.float32) * scale * loudness
    return jnp.minimum(jnp.maximum(result, -limit), limit).astype(held_as)


def setup_inputs(seed: int = 0) -> dict:
    seeds = jax.random.split(jax.random.key(seed), 20)
    stream = centred(seeds[0], (TOKENS, D), 1.0, 6.0, ((0, 32),))
    inner_act = centred(seeds[1], (TOKENS, D_INNER), 1.0, 6.0, ((0, 32), (1, 16)))
    gate_act = centred(seeds[2], (TOKENS, D_INNER), 1.0, 6.0, ((0, 32), (1, 16)))
    state_write = centred(seeds[3], (TOKENS, GROUPS, STATE), 1.0, 6.0, ((0, 32), (1, 16)))
    state_read = centred(seeds[4], (TOKENS, GROUPS, STATE), 1.0, 6.0, ((0, 32), (1, 16)))
    step_raw = draw_step_raw(jax.random.fold_in(seeds[19], 71), 0)
    conv_inner = centred(seeds[6], (CONV, D_INNER), 0.5, 3.0, ((1, 16),))
    conv_write = centred(seeds[7], (CONV, GROUPS, STATE), 0.5, 3.0, ((1, 16),))
    conv_read = centred(seeds[8], (CONV, GROUPS, STATE), 0.5, 3.0, ((1, 16),))
    step_bias = jnp.clip(jax.random.uniform(seeds[9], (HEADS,), jnp.float32, -0.5, 0.5) * level_of(seeds[9], (HEADS,), ((0, 16),), -0.4, 0.0), -0.5, 0.5)
    decay_log = draw_decay_log(jax.random.fold_in(seeds[19], 71), 0)
    inner_gain = jnp.clip(1.0 + 0.18 * jax.random.normal(seeds[11], (D_INNER,), jnp.float32), 0.1, 1.9)
    out_weight = centred(seeds[12], (D_INNER, D), D_INNER ** -0.5, 0.09375, ((0, 16),))
    ffn_gain = jnp.clip(1.0 + 0.18 * jax.random.normal(seeds[13], (D,), jnp.float32), 0.1, 1.9)
    expert_ids_keys = jax.random.split(jax.random.fold_in(seeds[14], 1), TOKENS // TOK_SP)
    expert_ids_turns = jax.random.permutation(jax.random.fold_in(seeds[14], 3), TOKENS // TOK_SP)
    expert_ids = jax.vmap(lambda own, number: routed_block(jax.random.fold_in(seeds[14], 2), own, number, TOK_SP, EXPERTS, TOPK, CAP, 1))(expert_ids_keys, expert_ids_turns).reshape((TOKENS, TOPK))
    expert_weights = jnp.clip(0.1 + 0.9 * jax.random.uniform(seeds[15], (TOKENS, TOPK), jnp.float32) ** level_of(seeds[15], (TOKENS, TOPK), ((0, 32),), -0.2, 0.2), 0.1, 1.0)
    expert_gate = centred(seeds[16], (EXPERTS, D, FF), D ** -0.5, 0.125, ((0, 32), (2, 16)))
    expert_up = centred(seeds[17], (EXPERTS, D, FF), D ** -0.5, 0.125, ((0, 32), (2, 16)))
    expert_down = centred(seeds[18], (EXPERTS, FF, D), FF ** -0.5, 0.1875, ((0, 32), (2, 16)))
    return {"stream": stream, "inner_act": inner_act, "gate_act": gate_act, "state_write": state_write, "state_read": state_read, "step_raw": step_raw, "conv_inner": conv_inner, "conv_write": conv_write, "conv_read": conv_read, "step_bias": step_bias, "decay_log": decay_log, "inner_gain": inner_gain, "out_weight": out_weight, "ffn_gain": ffn_gain, "expert_ids": expert_ids, "expert_weights": expert_weights, "expert_gate": expert_gate, "expert_up": expert_up, "expert_down": expert_down}


HIGH = lax.Precision.HIGHEST
EPS = 1e-06

def conv_silu(padded, weights, length):
    running = jnp.zeros((length, padded.shape[1]), jnp.float32)
    for offset in range(weights.shape[0]):
        running = running + weights[offset][None, :] * padded[offset:offset + length]
    return jax.nn.silu(running)

def block_terms(values, step_len, decay_rate, writes, reads, block_len):
    blocks = values.shape[0] // block_len
    groups, per_group, head_dim = (values.shape[1], values.shape[2], values.shape[3])
    state_dim = writes.shape[2]
    value_blk = values.reshape(blocks, block_len, groups, per_group, head_dim)
    step_blk = step_len.reshape(blocks, block_len, groups, per_group)
    write_blk = writes.reshape(blocks, block_len, groups, state_dim)
    read_blk = reads.reshape(blocks, block_len, groups, state_dim)
    cumul = jnp.cumsum(step_blk * decay_rate, axis=1)
    causal = jnp.tril(jnp.ones((block_len, block_len), dtype=bool))[None, :, :, None, None]
    spread = cumul[:, :, None] - cumul[:, None, :]
    within = jnp.where(causal, jnp.exp(jnp.where(causal, spread, 0.0)), 0.0)
    intersect = jnp.einsum('clgn,csgn->clsg', read_blk, write_blk, precision=HIGH)
    mixing = intersect[..., None] * within * step_blk[:, None]
    inside = jnp.einsum('clsgh,csghp->clghp', mixing, value_blk, precision=HIGH)
    to_end = jnp.exp(cumul[:, -1:] - cumul) * step_blk
    block_state = jnp.einsum('clgn,clghp->cghpn', write_blk, to_end[..., None] * value_blk, precision=HIGH)
    block_decay = jnp.exp(cumul[:, -1])

    def advance(carried, inputs):
        state_here, decay_here = inputs
        return (carried * decay_here[..., None, None] + state_here, carried)
    initial = jnp.zeros(block_state.shape[1:], jnp.float32)
    closing, entering = lax.scan(advance, initial, (block_state, block_decay))
    return (inside, entering, cumul, read_blk, closing)

def convolve(source, kernel):
    channels = source.shape[1]
    padded = jnp.concatenate([jnp.zeros((CONV - 1, channels), jnp.float32), source.astype(jnp.float32)], axis=0)
    return conv_silu(padded, kernel.astype(jnp.float32).reshape(CONV, channels), TOKENS)

def reference(stream, inner_act, gate_act, state_write, state_read, step_raw, conv_inner, conv_write, conv_read, step_bias, decay_log, inner_gain, out_weight, ffn_gain, expert_ids, expert_weights, expert_gate, expert_up, expert_down):
    per_group = HEADS // GROUPS
    write_width = GROUPS * STATE
    values = convolve(inner_act, conv_inner).reshape(TOKENS, GROUPS, per_group, HEADDIM)
    writes = convolve(state_write.reshape(TOKENS, write_width), conv_write).reshape(TOKENS, GROUPS, STATE)
    reads = convolve(state_read.reshape(TOKENS, write_width), conv_read).reshape(TOKENS, GROUPS, STATE)
    step_len = jax.nn.softplus(step_raw.astype(jnp.float32) + step_bias[None, :]).reshape(TOKENS, GROUPS, per_group)
    decay_rate = (-jnp.exp(decay_log)).reshape(GROUPS, per_group)
    inside, entering, cumul, read_blk, closing = block_terms(values, step_len, decay_rate, writes, reads, BLOCK)
    outside = jnp.einsum('clgn,cghpn->clghp', read_blk, entering, precision=HIGH) * jnp.exp(cumul)[..., None]
    gated = (inside + outside).reshape(TOKENS, D_INNER) * jax.nn.silu(gate_act.astype(jnp.float32))
    per_head = gated.reshape(TOKENS, HEADS, HEADDIM)
    per_head = per_head * lax.rsqrt(lax.optimization_barrier(jnp.mean(per_head * per_head, axis=-1, keepdims=True)) + EPS)
    mixed_inner = (per_head.reshape(TOKENS, D_INNER) * inner_gain[None, :]).astype(jnp.bfloat16)
    block_width = D_INNER // N_TP

    def add_block(index, running):
        begin = (index * block_width).astype(jnp.int32)
        columns = lax.dynamic_slice_in_dim(mixed_inner, begin, block_width, 1)
        weight_rows = lax.dynamic_slice_in_dim(out_weight, begin, block_width, 0)
        partial_value = jnp.dot(columns, weight_rows, preferred_element_type=jnp.float32).astype(jnp.bfloat16)
        partial_value = lax.optimization_barrier(partial_value)
        return running + partial_value.astype(jnp.float32)
    projected = lax.fori_loop(0, N_TP, add_block, jnp.zeros((TOKENS, D), jnp.float32))
    middle = stream.astype(jnp.float32) + projected
    normed = (middle * lax.rsqrt(lax.optimization_barrier(jnp.mean(middle * middle, axis=-1, keepdims=True)) + EPS) * ffn_gain[None, :]).astype(jnp.bfloat16)
    per_block = TOK_SP * TOPK
    choices_blk = expert_ids.reshape(N_SP, per_block)
    onehot = (choices_blk[..., None] == jnp.arange(EXPERTS, dtype=jnp.int32)[None, None, :]).astype(jnp.int32)
    earlier_count = jnp.cumsum(onehot, axis=1) - onehot
    slot_of = lax.optimization_barrier(jnp.sum(earlier_count * onehot, axis=-1))
    owner = jnp.arange(N_SP, dtype=jnp.int32)[:, None]
    target = (choices_blk * (N_SP * CAP) + owner * CAP + slot_of).reshape(-1).astype(jnp.int32)
    token_of = (jnp.arange(TOKENS * TOPK, dtype=jnp.int32) // TOPK).astype(jnp.int32)
    slot_table = jnp.full((EXPERTS * N_SP * CAP,), TOKENS, jnp.int32).at[target].set(token_of)
    slot_table = slot_table.reshape(EXPERTS, N_SP * CAP)
    padded_rows = jnp.concatenate([normed, jnp.zeros((1, D), jnp.bfloat16)], axis=0)

    def one_expert(index):
        tok_rows = padded_rows[slot_table[index]]
        gate_part = jnp.dot(tok_rows, expert_gate[index], preferred_element_type=jnp.float32)
        up_part = jnp.dot(tok_rows, expert_up[index], preferred_element_type=jnp.float32)
        hidden = (jax.nn.silu(gate_part) * up_part).astype(jnp.bfloat16)
        return jnp.dot(hidden, expert_down[index], preferred_element_type=jnp.float32).astype(jnp.bfloat16)
    results = lax.map(one_expert, jnp.arange(EXPERTS, dtype=jnp.int32))
    results = results.reshape(EXPERTS * N_SP * CAP, D)
    picked = results[target].astype(jnp.float32).reshape(TOKENS, TOPK, D)
    moe = lax.optimization_barrier(jnp.sum(picked * expert_weights[:, :, None], axis=1))
    return (middle + moe).astype(jnp.bfloat16)
```

```python
import functools

import jax
import jax.numpy as jnp
from jax import lax
from jax.experimental import pallas as pl
from jax.experimental.pallas import tpu as pltpu
from jax.sharding import PartitionSpec as P

F32 = jnp.float32
BF16 = jnp.bfloat16
HIGH = lax.Precision.HIGHEST
EPS = 1e-06
NSP = 32
NZ = 16
NTP = 16
CAP = 48
T = 384
D = 2048
INNER = 256
STATE = 128
HEADS = 4
HD = 64
SLOTS = NSP * CAP
COLS = D // NTP
FF = 1024


def dot(a, b, dims=((1,), (0,)), precision=None):
    return lax.dot_general(a, b, (dims, ((), ())), precision=precision, preferred_element_type=F32)


def iota(shape, dim):
    return lax.broadcasted_iota(jnp.int32, shape, dim)


def silu(v):
    return v / (1.0 + jnp.exp(-v))


def kernel(
    inner, gate, wr, rd, dtx, dtt, at, taps, prm, ow, stream, fgain, ids, idst, ew, wgu, wd,
    out,
    padf, halo_x, halo_w, halo_r, lam, rlam, spc, rs, es, re, mixed, pbuf, rp, kept, ssq, rss, scol,
    pm, q0, q1, sent, rx, xb, gu, dn, hid, ob, r3, r4,
    hs, hr, ls, lr, as_, ar, bs, br, ps, pr, ss, sr, ds_, dr, fs, fr, ts, tr, us, ur, gs, gr, loc,
):
    sp = lax.axis_index("sp")
    tp = lax.axis_index("tp")
    y = tp // 4
    x = lax.rem(tp, 4)
    z = sp // 2

    def rc(src, dst, send, recv, sp_to, tp_to):
        return pltpu.make_async_remote_copy(
            src_ref=src, dst_ref=dst, send_sem=send, recv_sem=recv,
            device_id={"sp": sp_to, "tp": tp_to}, device_id_type=pl.DeviceIdType.MESH,
        )

    def tp_of(y_, x_):
        return lax.rem(y_ + 4, 4) * 4 + lax.rem(x_ + 4, 4)

    def lanes(start, size):
        return pl.ds(pl.multiple_of(start, 128), size)

    barrier = pltpu.get_barrier_semaphore()

    def greet_sp(q, carry):
        pl.semaphore_signal(
            barrier, inc=1, device_id={"sp": lax.rem(sp + q, NSP), "tp": tp},
            device_id_type=pl.DeviceIdType.MESH,
        )
        return carry

    def greet_tp(q, carry):
        pl.semaphore_signal(
            barrier, inc=1, device_id={"sp": sp, "tp": lax.rem(tp + q, NTP)},
            device_id_type=pl.DeviceIdType.MESH,
        )
        return carry

    lax.fori_loop(1, NSP, greet_sp, 0)
    lax.fori_loop(1, NTP, greet_tp, 0)

    own = lanes(tp * COLS, COLS)
    local = [
        pltpu.make_async_copy(wgu, gu.at[:, own], loc.at[0]),
        pltpu.make_async_copy(wd, dn.at[:, own], loc.at[1]),
        pltpu.make_async_copy(stream.at[:, own], scol, loc.at[2]),
    ]
    for copy in local:
        copy.start()

    lower = iota((T, T), 0) > iota((T, T), 1)
    upper = iota((T, T), 0) < iota((T, T), 1)
    e0, e1 = ids[:, 0:1], ids[:, 1:2]
    lane_e = iota((T, 128), 1)
    oh0, oh1 = lane_e == e0, lane_e == e1
    both = jnp.where(oh0 | oh1, 1.0, 0.0).astype(BF16)
    count = dot(jnp.where(lower, 1.0, 0.0).astype(BF16), both)
    t0 = e0 * CAP + jnp.sum(jnp.where(oh0, count, 0.0), axis=1, keepdims=True).astype(jnp.int32)
    t1 = e1 * CAP + jnp.sum(jnp.where(oh1, count, 0.0), axis=1, keepdims=True).astype(jnp.int32)
    for c in range(0, SLOTS, 256):
        lane = iota((T, 256), 1) + c
        q0[:, c : c + 256] = jnp.where(lane == t0, 1.0, 0.0).astype(BF16)
        q1[:, c : c + 256] = jnp.where(lane == t1, 1.0, 0.0).astype(BF16)
    e0t, e1t = idst[0:1, :], idst[1:2, :]
    sub_e = iota((NSP, T), 0)
    oh0t, oh1t = sub_e == e0t, sub_e == e1t
    botht = jnp.where(oh0t | oh1t, 1.0, 0.0).astype(BF16)
    countt = dot(botht, jnp.where(upper, 1.0, 0.0).astype(BF16))
    t0t = e0t * CAP + jnp.sum(jnp.where(oh0t, countt, 0.0), axis=0, keepdims=True).astype(jnp.int32)
    t1t = e1t * CAP + jnp.sum(jnp.where(oh1t, countt, 0.0), axis=0, keepdims=True).astype(jnp.int32)
    for c in range(0, SLOTS, 256):
        row = iota((256, T), 0) + c
        pm[c : c + 256, :] = jnp.where((row == t0t) | (row == t1t), 1.0, 0.0).astype(BF16)

    ax = dtx[...] * prm[0:1, :]
    cumx = dot(jnp.where(upper, 0.0, 1.0), ax, precision=HIGH)
    cumt = dot(at[...], jnp.where(lower, 0.0, 1.0), precision=HIGH)
    total = cumx[T - 1 : T, :]
    lam[0:1, :] = total[:, :128]
    lam[1:2, :] = total[:, 128:]

    pl.semaphore_wait(barrier, NSP - 1 + NTP - 1)

    halos = [
        rc(ref.at[T - 16 : T], dst, hs.at[n], hr.at[n], lax.rem(sp + 1, NSP), tp)
        for n, (ref, dst) in enumerate(((inner, halo_x), (wr, halo_w), (rd, halo_r)))
    ]

    @pl.when(sp < NSP - 1)
    def _():
        for copy in halos:
            copy.start()

    def sp_order(i):
        step = (i + 1) // 2
        odd = lax.rem(i, 2)
        return lax.rem(sp + 16 + step * (2 * odd - 1), NSP)

    def sp_start(src_of, dst, send, recv):
        def body(i, carry):
            e = sp_order(i)
            rc(src_of(e), dst.at[sp], send.at[e], recv.at[sp], e, tp).start()
            return carry

        lax.fori_loop(0, NSP - 1, body, 0)

    def sp_wait(src_of, dst, send, recv):
        def body(i, carry):
            e = lax.rem(sp + 1 + i, NSP)
            copy = rc(src_of(e), dst.at[e], send.at[e], recv.at[e], e, tp)
            copy.wait_send()
            copy.wait_recv()
            return carry

        lax.fori_loop(0, NSP - 1, body, 0)

    sp_start(lambda e: lam, rlam, ls, lr)

    HALF = D // 2
    HALFD = FF // 2
    parts = {
        ("gu", 0): (gu, 0, HALF),
        ("gu", 1): (gu, HALF, HALF),
        ("dn", 0): (dn, 0, HALFD),
        ("dn", 1): (dn, HALFD, HALFD),
    }
    names = list(parts)

    def neighbour(axis, step):
        return tp_of(y, x + step) if axis == 0 else tp_of(y + step, x)

    def ring_first(name, start):
        buf, r, n = parts[name]
        copies = []
        for side, step in ((0, 1), (1, -1)):
            to = neighbour(name[1], step)
            ref = buf.at[r : r + n, own]
            k = names.index(name) * 16 + side
            copies.append(rc(ref, ref, gs.at[k], gr.at[k], sp, to))
        return copies

    def ring_second(name):
        buf, r, n = parts[name]
        copies = []
        for side, step in ((0, 1), (1, -1)):
            to = neighbour(name[1], step)
            origin = neighbour(name[1], -step)
            rr = r + side * (n // 2)
            ref = buf.at[rr : rr + n // 2, lanes(origin * COLS, COLS)]
            k = names.index(name) * 16 + 2 + side
            copies.append(rc(ref, ref, gs.at[k], gr.at[k], sp, to))
        return copies

    def line_slices(name, at_y, at_x):
        if name[1] == 0:
            return [lanes(lax.rem(at_y + 4, 4) * 512, 512)]
        return [lanes(tp_of(jnp.int32(k), at_x) * COLS, COLS) for k in range(4)]

    def ring_third(name):
        buf, r, n = parts[name]
        copies = []
        for side, step in ((0, 1), (1, -1)):
            to = neighbour(1 - name[1], step)
            for j, sl in enumerate(line_slices(name, y, x)):
                ref = buf.at[r : r + n, sl]
                k = names.index(name) * 16 + 4 + side * 2
                k = ("third", name, side, j)
                copies.append(rc(ref, ref, gs.at[sem_of(k)], gr.at[sem_of(k)], sp, to))
        return copies

    def ring_fourth(name):
        buf, r, n = parts[name]
        copies = []
        for side, step in ((0, 1), (1, -1)):
            to = neighbour(1 - name[1], step)
            rr = r + side * (n // 2)
            oy, ox = (y - step, x) if name[1] == 0 else (y, x - step)
            for j, sl in enumerate(line_slices(name, oy, ox)):
                ref = buf.at[rr : rr + n // 2, sl]
                k = ("fourth", name, side, j)
                copies.append(rc(ref, ref, gs.at[sem_of(k)], gr.at[sem_of(k)], sp, to))
        return copies

    table = {}

    def sem_of(key):
        if key not in table:
            table[key] = 64 + len(table)
        return table[key]

    def start(copies):
        for copy in copies:
            copy.start()

    def recv(copies):
        for copy in copies:
            copy.wait_recv()

    def send_done(copies):
        for copy in copies:
            copy.wait_send()

    for copy in local:
        copy.wait()
    first = [c for name in names for c in ring_first(name, True)]
    start(first)

    padf[8:, :] = jnp.concatenate([inner[...], wr[...], rd[...]], axis=1).astype(F32)

    @pl.when(sp > 0)
    def _():
        for copy in halos:
            copy.wait_recv()
        tail = jnp.concatenate([halo_x[...], halo_w[...], halo_r[...]], axis=1).astype(F32)
        padf[0:8, :] = tail[8:, :]

    @pl.when(sp == 0)
    def _():
        padf[0:8, :] = jnp.zeros((8, INNER + 2 * STATE), F32)

    conv = taps[0:1, :] * padf[5 : 5 + T, :]
    for k in range(1, 4):
        conv = conv + taps[k : k + 1, :] * padf[5 + k : 5 + k + T, :]
    conv = silu(conv)
    xs = conv[:, :INNER]
    bwb = conv[:, INNER : INNER + STATE].astype(BF16)
    crb = conv[:, INNER + STATE :].astype(BF16)

    recv(first)
    second = [c for name in names for c in ring_second(name)]
    start(second)

    weighted = (xs * (jnp.exp(total - cumx) * dtx[...])).astype(BF16)
    closing = dot(bwb, weighted, ((0,), (0,))).astype(BF16)
    spc[0:16] = closing[:, :128].reshape(16, 8, 128)
    spc[16:32] = closing[:, 128:].reshape(16, 8, 128)
    sp_start(lambda e: spc.at[e], rs, as_, ar)
    rs[pl.ds(sp, 1)] = spc[pl.ds(sp, 1)]
    rlam[pl.ds(sp, 1)] = lam[...].reshape(1, 2, 128)

    head_of = iota((1, INNER), 1) >> 6
    xsb = xs.astype(BF16)
    rows = 128
    insides = []
    for c in range(0, T, rows):
        n = c + rows
        g = dot(crb[c:n], bwb[:n], ((1,), (1,)))
        causal = iota((rows, n), 0) + c >= iota((rows, n), 1)
        acc = jnp.zeros((rows, INNER), F32)
        for h in range(HEADS):
            diff = cumx[c:n, h * HD : h * HD + 1] - cumt[h : h + 1, :n]
            w = jnp.where(causal, jnp.exp(jnp.minimum(diff, 0.0)), 0.0) * g * dtt[h : h + 1, :n]
            xh = jnp.where(head_of == h, xsb[:n], jnp.zeros((), BF16))
            acc = acc + dot(w.astype(BF16), xh)
        insides.append(acc)
    inside = jnp.concatenate(insides, axis=0)

    recv(second)
    third_gu = [c for name in names[:2] for c in ring_third(name)]
    start(third_gu)

    sp_wait(lambda e: lam, rlam, ls, lr)
    sp_wait(lambda e: spc.at[e], rs, as_, ar)
    half = sp // 16

    def scan(p, carry):
        es[pl.ds(p, 1)] = carry.astype(BF16).reshape(1, 8, 128)
        decay = jnp.exp(rlam[p, pl.ds(half, 1), :])
        return carry * decay + rs[p].astype(F32)

    lax.fori_loop(0, NSP, scan, jnp.zeros((8, 128), F32))
    sp_start(lambda e: es.at[e], re, bs, br)
    re[pl.ds(sp, 1)] = es[pl.ds(sp, 1)]
    gact = silu(gate[...].astype(F32))
    grow = jnp.exp(cumx)
    sp_wait(lambda e: es.at[e], re, bs, br)
    entering = jnp.concatenate(
        [re[0:16].astype(F32).reshape(128, 128), re[16:32].astype(F32).reshape(128, 128)], axis=1
    ).astype(BF16)
    gated = (inside + dot(crb, entering) * grow) * gact
    same = jnp.where((iota((INNER, INNER), 0) >> 6) == (iota((INNER, INNER), 1) >> 6), 1.0, 0.0)
    square = dot(gated * gated, same, precision=HIGH) * (1.0 / HD)
    mixed[...] = (gated * lax.rsqrt(square + EPS) * prm[1:2, :]).astype(BF16)

    for i in range(0, NTP, 2):
        term = dot(mixed[...], ow[:, i * COLS : (i + 2) * COLS]).astype(BF16)
        pbuf[i] = term[:, :COLS]
        pbuf[i + 1] = term[:, COLS:]

    def tp_start(src_of, dst_of, send, recv_, first_=1):
        def body(i, carry):
            j = lax.rem(tp + i, NTP)
            rc(src_of(j), dst_of(tp), send.at[j], recv_.at[tp], sp, j).start()
            return carry

        lax.fori_loop(1, NTP, body, 0)

    def tp_wait(src_of, dst_of, send, recv_):
        def body(i, carry):
            j = lax.rem(tp + i, NTP)
            copy = rc(src_of(j), dst_of(j), send.at[j], recv_.at[j], sp, j)
            copy.wait_send()
            copy.wait_recv()
            return carry

        lax.fori_loop(1, NTP, body, 0)

    tp_start(lambda j: pbuf.at[j], lambda j: rp.at[j], ps, pr)
    rp[pl.ds(tp, 1)] = pbuf[pl.ds(tp, 1)]
    tp_wait(lambda j: pbuf.at[j], lambda j: rp.at[j], ps, pr)
    middle = rp[0].astype(F32)
    for i in range(1, NTP):
        middle = middle + rp[i].astype(F32)
    middle = scol[...].astype(F32) + middle
    kept[...] = middle

    ssq[...] = dot(jnp.ones((8, COLS), F32), middle * middle, ((1,), (1,)), HIGH)
    tp_start(lambda j: ssq, lambda j: rss.at[j], ss, sr)
    rss[pl.ds(tp, 1)] = ssq[...].reshape(1, 8, T)
    recv(third_gu)
    fourth_gu = [c for name in names[:2] for c in ring_fourth(name)]
    third_dn = [c for name in names[2:] for c in ring_third(name)]
    tp_wait(lambda j: ssq, lambda j: rss.at[j], ss, sr)
    start(fourth_gu)
    start(third_dn)
    sums = rss[0]
    for i in range(1, NTP):
        sums = sums + rss[i]
    scale = jnp.transpose(lax.rsqrt(sums * (1.0 / D) + EPS))[:, 0:1]
    normed = (middle * scale * fgain[:, own]).astype(BF16)
    for e in range(0, NSP, 4):
        picked = dot(pm[e * CAP : (e + 4) * CAP, :], normed).astype(BF16)
        sent[e : e + 4] = picked.reshape(4, CAP, COLS)

    sp_start(lambda e: sent.at[e], rx, ds_, dr)
    rx[pl.ds(sp, 1)] = sent[pl.ds(sp, 1)]

    def chip_order(i):
        step = (i + 1) // 2
        odd = lax.rem(i, 2)
        return lax.rem(z + step * (2 * odd - 1) + NZ, NZ)

    def forward(i, carry):
        c = chip_order(i)
        for k in range(2):
            s = 2 * c + k

            @pl.when(s != sp)
            def _():
                copy = rc(sent.at[s], rx.at[s], ds_.at[s], dr.at[s], s, tp)
                copy.wait_send()
                copy.wait_recv()

        src = rx.at[pl.ds(2 * c, 2)]

        @pl.when(c != tp)
        def _():
            rc(src, xb.at[:, :, own], fs.at[c], fr.at[tp], sp, c).start()

        @pl.when(c == tp)
        def _():
            xb[:, :, own] = rx[pl.ds(2 * c, 2)]

        return carry

    lax.fori_loop(0, NZ, forward, 0)
    recv(third_dn)
    fourth_dn = [c for name in names[2:] for c in ring_fourth(name)]
    start(fourth_dn)
    tp_wait(
        lambda j: rx.at[pl.ds(2 * j, 2)],
        lambda j: xb.at[:, :, lanes(j * COLS, COLS)],
        fs, fr,
    )
    recv(fourth_gu)

    xrow = xb[...].reshape(2 * CAP, D)
    low = iota((1, 128), 1) < 64

    def expert_in(i, carry):
        g = dot(xrow, gu[:, lanes(i * 256, 256)])
        a, b = g[:, :128], g[:, 128:]
        even = silu(a) * pltpu.roll(a, 64, 1)
        odd = silu(b) * pltpu.roll(b, 64, 1)
        hid[:, lanes(i * 128, 128)] = jnp.where(low, even, odd).astype(BF16)
        return carry

    lax.fori_loop(0, NTP // 2, expert_in, 0)
    recv(fourth_dn)
    hrow = hid[...]

    def expert_out(i, carry):
        o = dot(hrow, dn[:, lanes(i * 256, 256)]).astype(BF16)
        ob[:, :, lanes(i * 256, 256)] = o.reshape(2, CAP, 256)
        return carry

    lax.fori_loop(0, D // 256, expert_out, 0)

    tp_start(lambda j: ob.at[:, :, lanes(j * COLS, COLS)], lambda j: r3.at[j], ts, tr)
    r3[pl.ds(tp, 1)] = ob[:, :, own].reshape(1, 2, CAP, COLS)

    def give_back(i, carry):
        c = chip_order(NZ - 1 - i)

        @pl.when(c != tp)
        def _():
            copy = rc(ob.at[:, :, lanes(c * COLS, COLS)], r3.at[c], ts.at[c], tr.at[c], sp, c)
            copy.wait_send()
            copy.wait_recv()

        for k in range(2):
            s = 2 * c + k

            @pl.when(s != sp)
            def _():
                rc(r3.at[c, k], r4.at[sp], us.at[s], ur.at[sp], s, tp).start()

            @pl.when(s == sp)
            def _():
                r4[pl.ds(sp, 1)] = r3[c, pl.ds(k, 1)]

        return carry

    lax.fori_loop(0, NZ, give_back, 0)
    sp_wait(lambda e: r3.at[e // 2, lax.rem(e, 2)], r4, us, ur)

    results = r4[...].reshape(SLOTS, COLS)
    moe = dot(q0[...], results) * ew[:, 0:1] + dot(q1[...], results) * ew[:, 1:2]
    out[...] = (kept[...] + moe).astype(BF16)

    @pl.when(sp < NSP - 1)
    def _():
        for copy in halos:
            copy.wait_send()

    for copies in (first, second, third_gu, third_dn, fourth_gu, fourth_dn):
        send_done(copies)


def per_device(
    stream, inner_act, gate_act, state_write, state_read, step_raw, conv_inner, conv_write,
    conv_read, step_bias, decay_log, inner_gain, out_weight, ffn_gain, expert_ids,
    expert_weights, expert_gate, expert_up, expert_down,
):
    dt = jax.nn.softplus(step_raw.astype(F32) + step_bias[None, :])
    rate = -jnp.exp(decay_log)
    dtx = jnp.repeat(dt, HD, axis=1)
    dtt = jnp.zeros((8, T), F32).at[:HEADS].set(dt.T)
    at = jnp.zeros((8, T), F32).at[:HEADS].set((dt * rate[None, :]).T)
    taps = jnp.concatenate(
        [conv_inner, conv_write.reshape(4, STATE), conv_read.reshape(4, STATE)], axis=1
    ).astype(F32)
    prm = jnp.stack([jnp.repeat(rate, HD), inner_gain])
    idst = jnp.zeros((8, T), jnp.int32).at[:2].set(expert_ids.T)
    gate_w, up_w = expert_gate[0], expert_up[0]
    odd = lax.rem(lax.axis_index("tp"), 2) == 1
    wgu = jnp.concatenate([jnp.where(odd, up_w, gate_w), jnp.where(odd, gate_w, up_w)], axis=1)
    vmem = pl.BlockSpec(memory_space=pltpu.VMEM)
    hbm = pl.BlockSpec(memory_space=pl.ANY)
    dma = pltpu.SemaphoreType.DMA
    return pl.pallas_call(
        kernel,
        name="layer",
        out_shape=jax.ShapeDtypeStruct((T, COLS), BF16),
        in_specs=[vmem] * 10 + [hbm] + [vmem] * 4 + [hbm] * 2,
        out_specs=vmem,
        scratch_shapes=[
            pltpu.VMEM((T + 8, INNER + 2 * STATE), F32),
            pltpu.VMEM((16, INNER), BF16),
            pltpu.VMEM((16, STATE), BF16),
            pltpu.VMEM((16, STATE), BF16),
            pltpu.VMEM((2, 128), F32),
            pltpu.VMEM((NSP, 2, 128), F32),
            pltpu.VMEM((NSP, 8, 128), BF16),
            pltpu.VMEM((NSP, 8, 128), BF16),
            pltpu.VMEM((NSP, 8, 128), BF16),
            pltpu.VMEM((NSP, 8, 128), BF16),
            pltpu.VMEM((T, INNER), BF16),
            pltpu.VMEM((NTP, T, COLS), BF16),
            pltpu.VMEM((NTP, T, COLS), BF16),
            pltpu.VMEM((T, COLS), F32),
            pltpu.VMEM((8, T), F32),
            pltpu.VMEM((NTP, 8, T), F32),
            pltpu.VMEM((T, COLS), BF16),
            pltpu.VMEM((SLOTS, T), BF16),
            pltpu.VMEM((T, SLOTS), BF16),
            pltpu.VMEM((T, SLOTS), BF16),
            pltpu.VMEM((NSP, CAP, COLS), BF16),
            pltpu.VMEM((NSP, CAP, COLS), BF16),
            pltpu.VMEM((2, CAP, D), BF16),
            pltpu.VMEM((D, D), BF16),
            pltpu.VMEM((FF, D), BF16),
            pltpu.VMEM((2 * CAP, FF), BF16),
            pltpu.VMEM((2, CAP, D), BF16),
            pltpu.VMEM((NTP, 2, CAP, COLS), BF16),
            pltpu.VMEM((NSP, CAP, COLS), BF16),
            dma((3,)), dma((3,)),
            dma((NSP,)), dma((NSP,)),
            dma((NSP,)), dma((NSP,)),
            dma((NSP,)), dma((NSP,)),
            dma((NTP,)), dma((NTP,)),
            dma((NTP,)), dma((NTP,)),
            dma((NSP,)), dma((NSP,)),
            dma((NTP,)), dma((NTP,)),
            dma((NTP,)), dma((NTP,)),
            dma((NSP,)), dma((NSP,)),
            dma((112,)), dma((112,)),
            dma((3,)),
        ],
        compiler_params=pltpu.CompilerParams(
            collective_id=0, has_side_effects=True, vmem_limit_bytes=60 * 1024 * 1024
        ),
    )(
        inner_act, gate_act, state_write.reshape(T, STATE), state_read.reshape(T, STATE),
        dtx, dtt, at, taps, prm, out_weight, stream, ffn_gain.reshape(1, D), expert_ids, idst,
        expert_weights, wgu, expert_down[0],
    )


def solution(mesh):
    return jax.shard_map(
        per_device,
        mesh=mesh,
        in_specs=(
            P("sp", None), P("sp", "tp"), P("sp", "tp"), P("sp", "tp", None), P("sp", "tp", None),
            P("sp", "tp"), P(None, "tp"), P(None, "tp", None), P(None, "tp", None), P("tp"),
            P("tp"), P("tp"), P("tp", None), P(), P("sp", None), P("sp", None),
            P("sp", None, "tp"), P("sp", None, "tp"), P("sp", None, "tp"),
        ),
        out_specs=P("sp", "tp"),
        check_vma=False,
    )
```

```python
import functools

import jax
import jax.numpy as jnp
from jax import lax
from jax.experimental import pallas as pl
from jax.experimental.pallas import tpu as pltpu
from jax.sharding import PartitionSpec as P

F32 = jnp.float32
BF16 = jnp.bfloat16
HIGH = lax.Precision.HIGHEST
EPS = 1e-06
NSP = 32
NZ = 16
NTP = 16
CAP = 48
T = 384
D = 2048
INNER = 256
STATE = 128
HEADS = 4
HD = 64
SLOTS = NSP * CAP
COLS = D // NTP
FF = 1024


def dot(a, b, dims=((1,), (0,)), precision=None):
    return lax.dot_general(a, b, (dims, ((), ())), precision=precision, preferred_element_type=F32)


def iota(shape, dim):
    return lax.broadcasted_iota(jnp.int32, shape, dim)


def silu(v):
    return v / (1.0 + jnp.exp(-v))


def kernel(
    raw, bias, dlog, tap_x, tap_w, tap_r, again, fgain, ids, ew,
    inner_h, gate_h, wr_h, rd_h, ow_h, stream, wg, wu, wd,
    out,
    inner, gate, wr, rd, ow, padf, halo_x, halo_w, halo_r, lam, rlam, spc, rs, es, re, colbuf, mixed, pbuf, v1, w1b, z1, s1, v2, w2b, z2, kept, ssq, rss, scol,
    pm, q0, q1, sent, rx, xb, gu, dn, hid, ob, r3, r4,
    hs, hr, ls, lr, as_, ar, bs, br, ps, pr, ss, sr, ds_, dr, fs, fr, ts, tr, us, ur, gs, gr, loc,
):
    sp = lax.axis_index("sp")
    tp = lax.axis_index("tp")
    y = tp // 4
    x = lax.rem(tp, 4)
    z = sp // 2

    def rc(src, dst, send, recv, sp_to, tp_to):
        return pltpu.make_async_remote_copy(
            src_ref=src, dst_ref=dst, send_sem=send, recv_sem=recv,
            device_id={"sp": sp_to, "tp": tp_to}, device_id_type=pl.DeviceIdType.MESH,
        )

    def tp_of(y_, x_):
        return lax.rem(y_ + 4, 4) * 4 + lax.rem(x_ + 4, 4)

    def lanes(start, size):
        return pl.ds(pl.multiple_of(start, 128), size)

    barrier = pltpu.get_barrier_semaphore()

    def greet_sp(q, carry):
        pl.semaphore_signal(
            barrier, inc=1, device_id={"sp": lax.rem(sp + q, NSP), "tp": tp},
            device_id_type=pl.DeviceIdType.MESH,
        )
        return carry

    def greet_tp(q, carry):
        pl.semaphore_signal(
            barrier, inc=1, device_id={"sp": sp, "tp": lax.rem(tp + q, NTP)},
            device_id_type=pl.DeviceIdType.MESH,
        )
        return carry

    lax.fori_loop(1, NSP, greet_sp, 0)
    lax.fori_loop(1, NTP, greet_tp, 0)

    own = lanes(tp * COLS, COLS)
    odd = lax.rem(tp, 2)
    local = [
        pltpu.make_async_copy(wg, gu.at[y, x, pl.ds(odd * 64, 64)], loc.at[0]),
        pltpu.make_async_copy(wu, gu.at[y, x, pl.ds(64 - odd * 64, 64)], loc.at[1]),
        pltpu.make_async_copy(wd, dn.at[y, x], loc.at[2]),
        pltpu.make_async_copy(inner_h, inner, loc.at[3]),
        pltpu.make_async_copy(wr_h, wr, loc.at[4]),
        pltpu.make_async_copy(rd_h, rd, loc.at[5]),
        pltpu.make_async_copy(gate_h, gate, loc.at[6]),
        pltpu.make_async_copy(ow_h, ow, loc.at[7]),
        pltpu.make_async_copy(stream.at[:, own], scol, loc.at[8]),
    ]
    for copy in local:
        copy.start()

    rate = -jnp.exp(dlog[...])
    step = raw[...].astype(F32)
    step = jnp.concatenate([step[h : h + 1] + bias[0:1, h : h + 1] for h in range(HEADS)], axis=0)
    dtt = jnp.maximum(step, 0.0) + jnp.log1p(jnp.exp(-jnp.abs(step)))
    at = jnp.concatenate(
        [dtt[h : h + 1] * rate[0:1, h : h + 1] for h in range(HEADS)] + [jnp.zeros((4, T), F32)], axis=0
    )
    colbuf[0:4, :] = dtt
    colbuf[4:6, :] = ids[...].astype(F32)
    colbuf[6:8, :] = ew[...]
    cols = jnp.transpose(colbuf[...])
    e0, e1 = cols[:, 4:5].astype(jnp.int32), cols[:, 5:6].astype(jnp.int32)
    w0, w1 = cols[:, 6:7], cols[:, 7:8]
    head_of = iota((1, INNER), 1) >> 6

    def by_head(pick):
        v = jnp.where(head_of == 0, pick(0), pick(1))
        return jnp.where(head_of == 3, pick(3), jnp.where(head_of == 2, pick(2), v))

    dtx = by_head(lambda h: cols[:, h : h + 1])
    ratex = by_head(lambda h: rate[0:1, h : h + 1])

    lower = iota((T, T), 0) > iota((T, T), 1)
    upper = iota((T, T), 0) < iota((T, T), 1)
    ax = dtx * ratex
    cumx = dot(jnp.where(upper, 0.0, 1.0), ax, precision=HIGH)
    cumt = dot(at, jnp.where(lower, 0.0, 1.0), precision=HIGH)
    total = cumx[T - 1 : T, :]
    lam[0:1, :] = total[:, :128]
    lam[1:2, :] = total[:, 128:]

    with jax.named_scope("w_barrier"):
        pl.semaphore_wait(barrier, NSP - 1 + NTP - 1)

    for copy in local[3:6]:
        copy.wait()

    halos = [
        rc(ref.at[T - 16 : T], dst, hs.at[n], hr.at[n], lax.rem(sp + 1, NSP), tp)
        for n, (ref, dst) in enumerate(((inner, halo_x), (wr, halo_w), (rd, halo_r)))
    ]

    @pl.when(sp < NSP - 1)
    def _():
        for copy in halos:
            copy.start()

    def sp_order(i):
        step = (i + 1) // 2
        odd = lax.rem(i, 2)
        return lax.rem(sp + 16 + step * (2 * odd - 1), NSP)

    def took(ref, send=None, recv=None):
        copy = rc(ref, ref, send, recv, sp, tp) if send is not None and recv is not None else None
        if copy is None:
            sem = send if send is not None else recv
            copy = rc(ref, ref, sem, sem, sp, tp)
        if send is not None:
            copy.wait_send()
        if recv is not None:
            copy.wait_recv()

    def sp_start(src_of, dst, send, recv):
        def body(i, carry):
            e = sp_order(i)
            rc(src_of(e), dst.at[sp], send.at[0], recv.at[0], e, tp).start()
            return carry

        lax.fori_loop(0, NSP - 1, body, 0)

    def sp_wait(dst, send, recv, name):
        with jax.named_scope(name):
            took(dst.at[0 : NSP - 1], send.at[0], recv.at[0])

    sp_start(lambda e: lam, rlam, ls, lr)

    half_rows = {0: COLS // 2, 1: FF // 2}

    def neighbour(axis, step):
        return tp_of(y, x + step) if axis == 0 else tp_of(y + step, x)

    def shard(buf, j, first, rows):
        return buf.at[j // 4, lax.rem(j, 4), pl.ds(first, rows)]

    def line(buf, axis, at_y, at_x, first, rows):
        if axis == 0:
            return buf.at[lax.rem(at_y + 4, 4), :, pl.ds(first, rows)]
        return buf.at[:, lax.rem(at_x + 4, 4), pl.ds(first, rows)]

    def ring(which, axis, stage, quarter=None):
        buf, n = ((gu, dn)[which], half_rows[which])
        base = axis * n
        copies = []
        for side, step in ((0, 1), (1, -1)):
            k = which * 4 + stage if quarter is None else 8 + quarter
            part = (base + side * (n // 2), n // 2) if stage % 2 else (base, n)
            if quarter is not None:
                part = (base + quarter * (n // 4), n // 4)
            if stage < 2:
                to = neighbour(axis, step)
                ref = shard(buf, tp if stage == 0 else neighbour(axis, -step), *part)
            else:
                to = neighbour(1 - axis, step)
                back = 0 if stage == 2 else step
                oy, ox = (y - back, x) if axis == 0 else (y, x - back)
                ref = line(buf, axis, oy, ox, *part)
            copies.append(rc(ref, ref, gs.at[k], gr.at[k], sp, to))
        return copies

    def rings(which, stage, quarter=None):
        return [c for axis in (0, 1) for c in ring(which, axis, stage, quarter)]

    def ring_bytes(which, stage, quarter=None):
        buf, n = ((gu, dn)[which], half_rows[which])
        rows_ = (n // 2 if stage % 2 else n) if quarter is None else n // 4
        if stage < 2:
            return buf.at[0, :, pl.ds(0, rows_)]
        return buf.at[:, :, pl.ds(0, rows_)]

    def ring_recv(which, stage, quarter=None):
        k = which * 4 + stage if quarter is None else 8 + quarter
        took(ring_bytes(which, stage, quarter), recv=gr.at[k])

    def ring_sent(which, stage, quarter=None):
        k = which * 4 + stage if quarter is None else 8 + quarter
        took(ring_bytes(which, stage, quarter), send=gs.at[k])

    def start(copies):
        for copy in copies:
            copy.start()

    for copy in local[:3]:
        copy.wait()
    first_gu, first_dn = rings(0, 0), rings(1, 0)
    start(first_gu)
    start(first_dn)

    padf[8:, :] = jnp.concatenate([inner[...], wr[...], rd[...]], axis=1).astype(F32)

    @pl.when(sp > 0)
    def _():
        for copy in halos:
            copy.wait_recv()
        tail = jnp.concatenate([halo_x[...], halo_w[...], halo_r[...]], axis=1).astype(F32)
        padf[0:8, :] = tail[8:, :]

    @pl.when(sp == 0)
    def _():
        padf[0:8, :] = jnp.zeros((8, INNER + 2 * STATE), F32)

    taps = jnp.concatenate([tap_x[...], tap_w[...], tap_r[...]], axis=1).astype(F32)
    conv = taps[0:1, :] * padf[5 : 5 + T, :]
    for k in range(1, 4):
        conv = conv + taps[k : k + 1, :] * padf[5 + k : 5 + k + T, :]
    conv = silu(conv)
    xs = conv[:, :INNER]
    bwb = conv[:, INNER : INNER + STATE].astype(BF16)
    crb = conv[:, INNER + STATE :].astype(BF16)

    weighted = (xs * (jnp.exp(total - cumx) * dtx)).astype(BF16)
    closing = dot(bwb, weighted, ((0,), (0,))).astype(BF16)
    spc[0:16] = closing[:, :128].reshape(16, 8, 128)
    spc[16:32] = closing[:, 128:].reshape(16, 8, 128)
    sp_start(lambda e: spc.at[e], rs, as_, ar)
    rs[pl.ds(sp, 1)] = spc[pl.ds(sp, 1)]
    rlam[pl.ds(sp, 1)] = lam[...].reshape(1, 2, 128)

    xsb = xs.astype(BF16)
    rows = 128
    insides = []
    for c in range(0, T, rows):
        n = c + rows
        g = dot(crb[c:n], bwb[:n], ((1,), (1,)))
        causal = iota((rows, n), 0) + c >= iota((rows, n), 1)
        acc = jnp.zeros((rows, INNER), F32)
        for h in range(HEADS):
            diff = cumx[c:n, h * HD : h * HD + 1] - cumt[h : h + 1, :n]
            w = jnp.where(causal, jnp.exp(jnp.minimum(diff, 0.0)), 0.0) * g * dtt[h : h + 1, :n]
            xh = jnp.where(head_of == h, xsb[:n], jnp.zeros((), BF16))
            acc = acc + dot(w.astype(BF16), xh)
        insides.append(acc)
    inside = jnp.concatenate(insides, axis=0)

    with jax.named_scope("w_first_gu"):
        ring_recv(0, 0)
    start(rings(0, 1))
    with jax.named_scope("w_first_dn"):
        ring_recv(1, 0)
    start(rings(1, 1))

    lane_e = iota((T, 128), 1)
    oh0, oh1 = lane_e == e0, lane_e == e1
    both = jnp.where(oh0 | oh1, 1.0, 0.0).astype(BF16)
    count = dot(jnp.where(lower, 1.0, 0.0).astype(BF16), both)
    t0 = e0 * CAP + jnp.sum(jnp.where(oh0, count, 0.0), axis=1, keepdims=True).astype(jnp.int32)
    t1 = e1 * CAP + jnp.sum(jnp.where(oh1, count, 0.0), axis=1, keepdims=True).astype(jnp.int32)
    for c in range(0, SLOTS, 256):
        lane = iota((T, 256), 1) + c
        q0[:, c : c + 256] = jnp.where(lane == t0, 1.0, 0.0).astype(BF16)
        q1[:, c : c + 256] = jnp.where(lane == t1, 1.0, 0.0).astype(BF16)
    e0t, e1t = ids[0:1, :], ids[1:2, :]
    sub_e = iota((NSP, T), 0)
    oh0t, oh1t = sub_e == e0t, sub_e == e1t
    botht = jnp.where(oh0t | oh1t, 1.0, 0.0).astype(BF16)
    countt = dot(botht, jnp.where(upper, 1.0, 0.0).astype(BF16))
    t0t = e0t * CAP + jnp.sum(jnp.where(oh0t, countt, 0.0), axis=0, keepdims=True).astype(jnp.int32)
    t1t = e1t * CAP + jnp.sum(jnp.where(oh1t, countt, 0.0), axis=0, keepdims=True).astype(jnp.int32)
    for c in range(0, SLOTS, 256):
        row = iota((256, T), 0) + c
        pm[c : c + 256, :] = jnp.where((row == t0t) | (row == t1t), 1.0, 0.0).astype(BF16)

    with jax.named_scope("w_second_gu"):
        ring_recv(0, 1)
    start(rings(0, 2, 0))
    start(rings(0, 2, 1))
    sp_wait(rlam, ls, lr, "w_lam")
    sp_wait(rs, as_, ar, "w_state1")
    half = sp // 16

    def scan(p, carry):
        es[pl.ds(p, 1)] = carry.astype(BF16).reshape(1, 8, 128)
        decay = jnp.exp(rlam[p, pl.ds(half, 1), :])
        return carry * decay + rs[p].astype(F32)

    with jax.named_scope("scan"):
        lax.fori_loop(0, NSP, scan, jnp.zeros((8, 128), F32))
    sp_start(lambda e: es.at[e], re, bs, br)
    re[pl.ds(sp, 1)] = es[pl.ds(sp, 1)]
    for copy in local[6:]:
        copy.wait()
    gact = silu(gate[...].astype(F32))
    grow = jnp.exp(cumx)
    sp_wait(re, bs, br, "w_state2")
    entering = jnp.concatenate(
        [re[0:16].astype(F32).reshape(128, 128), re[16:32].astype(F32).reshape(128, 128)], axis=1
    ).astype(BF16)
    gated = (inside + dot(crb, entering) * grow) * gact
    same = jnp.where((iota((INNER, INNER), 0) >> 6) == (iota((INNER, INNER), 1) >> 6), 1.0, 0.0)
    square = dot(gated * gated, same, precision=HIGH) * (1.0 / HD)
    mixed[...] = (gated * lax.rsqrt(square + EPS) * again[...]).astype(BF16)

    for i in range(0, NTP, 2):
        term = dot(mixed[...], ow[:, i * COLS : (i + 2) * COLS]).astype(BF16)
        pbuf[i // 4, i % 4] = term[:, :COLS]
        pbuf[i // 4, i % 4 + 1] = term[:, COLS:]

    HALF = T // 2
    PART = T // 4

    def at4(v):
        return lax.rem(v + 4, 4)

    def place(h):
        return (x, y) if h == 0 else (y, x)

    def slab(h, pos, first, rows):
        if h == 0:
            return pbuf.at[:, at4(pos), pl.ds(h * HALF + first, rows)]
        return pbuf.at[at4(pos), :, pl.ds(h * HALF + first, rows)]

    def read(h, pos, first, rows):
        if h == 0:
            v = pbuf[:, pl.ds(at4(pos), 1), h * HALF + first : h * HALF + first + rows]
        else:
            v = pbuf[pl.ds(at4(pos), 1), :, h * HALF + first : h * HALF + first + rows]
        return v.reshape(4, rows, COLS).astype(F32)

    hops = [(h, side, step) for h in (0, 1) for side, step in ((0, 1), (1, -1))]

    def hop(kind, h, side, step, src, dst):
        axis = h if kind < 3 else 1 - h
        late = kind // 3
        k = late * 3 + (0 if kind % 3 == 0 else 1 + h)
        return rc(src, dst, ps.at[kind], pr.at[k], sp, neighbour(axis, step))

    relay1, own1, sum1, relay2, own2, sum2 = [], [], [], [], [], []
    for h, side, step in hops:
        p, _ = place(h)
        relay1.append(hop(0, h, side, step, slab(h, p + 2, side * PART, PART), v1.at[h, side]))
        part = pl.ds((1 - side) * PART, PART)
        own1.append(hop(1, h, side, step, slab(h, p + step, (1 - side) * PART, PART), w1b.at[h, side, :, part]))
        part = pl.ds(side * PART, PART)
        sum1.append(hop(2, h, side, step, z1.at[h, side], w1b.at[h, side, :, part]))
    start(relay1)
    start(own1)
    with jax.named_scope("w_relay1"):
        took(v1, recv=pr.at[0])
    for n, (h, side, step) in enumerate(hops):
        p, _ = place(h)
        z1[h, side] = (read(h, p + step, side * PART, PART) + v1[h, side].astype(F32)).astype(BF16)
        sum1[n].start()
    start(rings(0, 2, 2))
    for h in (0, 1):
        p, p2 = place(h)
        with jax.named_scope("w_sum1"):
            took(w1b.at[h], recv=pr.at[1 + h])
        sums4 = read(h, p, 0, HALF) + w1b[h, 0].astype(F32) + w1b[h, 1].astype(F32)
        s1[h] = sums4.astype(BF16)
        for side, step in ((0, 1), (1, -1)):
            first_, other = pl.ds(side * PART, PART), pl.ds((1 - side) * PART, PART)
            relay2.append(hop(3, h, side, step, s1.at[h, at4(p2 + 2), first_], v2.at[h, side]))
            own2.append(hop(4, h, side, step, s1.at[h, at4(p2 + step), other], w2b.at[h, side, other]))
            sum2.append(hop(5, h, side, step, z2.at[h, side], w2b.at[h, side, first_]))
        start(relay2[2 * h : 2 * h + 2])
        start(own2[2 * h : 2 * h + 2])
    with jax.named_scope("w_relay2"):
        took(v2, recv=pr.at[3])
    for n, (h, side, step) in enumerate(hops):
        _, p2 = place(h)
        here = s1[h, pl.ds(at4(p2 + step), 1), side * PART : (side + 1) * PART].reshape(PART, COLS)
        z2[h, side] = (here.astype(F32) + v2[h, side].astype(F32)).astype(BF16)
        sum2[n].start()
    start(rings(0, 2, 3))
    halves = []
    for h in (0, 1):
        p, p2 = place(h)
        with jax.named_scope("w_sum2"):
            took(w2b.at[h], recv=pr.at[4 + h])
        mine = pbuf[pl.ds(y, 1), pl.ds(x, 1), h * HALF : (h + 1) * HALF].reshape(HALF, COLS).astype(F32)
        for side in (0, 1):
            mine = mine + w1b[h, side, pl.ds(p2, 1)].reshape(HALF, COLS).astype(F32)
        halves.append(mine + w2b[h, 0].astype(F32) + w2b[h, 1].astype(F32))
    middle = scol[...].astype(F32) + jnp.concatenate(halves, axis=0)
    kept[...] = middle

    ssq[...] = dot(jnp.ones((8, COLS), F32), middle * middle, ((1,), (1,)), HIGH)
    def tell(i, carry):
        j = lax.rem(tp + i, NTP)
        rc(ssq, rss.at[tp], ss.at[0], sr.at[0], sp, j).start()
        return carry

    lax.fori_loop(1, NTP, tell, 0)
    rss[pl.ds(tp, 1)] = ssq[...].reshape(1, 8, T)
    with jax.named_scope("w_second_dn"):
        ring_recv(1, 1)
    start(rings(1, 2))
    with jax.named_scope("w_ssq"):
        took(rss.at[0 : NTP - 1], ss.at[0], sr.at[0])
    sums = rss[0]
    for i in range(1, NTP):
        sums = sums + rss[i]
    scale = jnp.transpose(lax.rsqrt(sums * (1.0 / D) + EPS))[:, 0:1]
    normed = (middle * scale * fgain[:, own]).astype(BF16)
    for e in range(0, NSP, 4):
        picked = dot(pm[e * CAP : (e + 4) * CAP, :], normed).astype(BF16)
        sent[e : e + 4] = picked.reshape(4, CAP, COLS)

    def dispatch(i, carry):
        e = sp_order(i)
        rc(sent.at[e], rx.at[sp], ds_.at[0], dr.at[z], e, tp).start()
        return carry

    lax.fori_loop(0, NSP - 1, dispatch, 0)
    rx[pl.ds(sp, 1)] = sent[pl.ds(sp, 1)]

    def chip_order(i):
        step = (i + 1) // 2
        odd = lax.rem(i, 2)
        return lax.rem(z + step * (2 * odd - 1) + NZ, NZ)

    def forward(i, carry):
        c = chip_order(NZ - 1 - i)
        @pl.when(c != z)
        def _():
            took(rx.at[pl.ds(2 * c, 2)], recv=dr.at[c])

        @pl.when(c == z)
        def _():
            took(rx.at[2 * c], recv=dr.at[c])

        src = rx.at[pl.ds(2 * c, 2)]

        @pl.when(c != tp)
        def _():
            rc(src, xb.at[:, :, own], fs.at[0], fr.at[0], sp, c).start()

        @pl.when(c == tp)
        def _():
            xb[:, :, own] = rx[pl.ds(2 * c, 2)]

        return carry

    with jax.named_scope("w_third_gu"):
        for q in range(4):
            ring_recv(0, 2, q)
    start(rings(0, 3))
    with jax.named_scope("forward"):
        lax.fori_loop(0, NZ, forward, 0)
    with jax.named_scope("w_third_dn"):
        ring_recv(1, 2)
    start(rings(1, 3))
    with jax.named_scope("w_fwd"):
        took(r3.at[0 : NTP - 1], fs.at[0], fr.at[0])
    with jax.named_scope("w_fourth_gu"):
        ring_recv(0, 3)

    xrow = xb[...].reshape(2 * CAP, D)
    low = iota((1, 128), 1) < 64

    def expert_in(i, carry):
        q = 2 * lax.rem(i, 2)
        w = gu[i // 2, pl.ds(q, 2)].reshape(256, D)
        g = dot(xrow, w, ((1,), (1,)))
        a, b = g[:, :128], g[:, 128:]
        even = silu(a) * pltpu.roll(a, 64, 1)
        odd = silu(b) * pltpu.roll(b, 64, 1)
        hid[:, lanes(i * 128, 128)] = jnp.where(low, even, odd).astype(BF16)
        return carry

    with jax.named_scope("expert_in"):
        lax.fori_loop(0, NTP // 2, expert_in, 0)
    with jax.named_scope("w_fourth_dn"):
        ring_recv(1, 3)
    hrow = hid[...]

    def expert_out(i, carry):
        i = lax.rem(i + tp // 2, NTP // 2)
        q = 2 * lax.rem(i, 2)
        w = jnp.concatenate([dn[i // 2, q], dn[i // 2, q + 1]], axis=1)
        o = dot(hrow, w).astype(BF16)
        ob[:, :, lanes(i * 256, 256)] = o.reshape(2, CAP, 256)
        for k in range(2):
            j = 2 * i + k

            @pl.when(j != tp)
            def _():
                rc(ob.at[:, :, lanes(j * COLS, COLS)], r3.at[tp], ts.at[0], tr.at[tp], sp, j).start()

        return carry

    with jax.named_scope("expert_out"):
        lax.fori_loop(0, D // 256, expert_out, 0)

    r3[pl.ds(tp, 1)] = ob[:, :, own].reshape(1, 2, CAP, COLS)

    def give_back(i, carry):
        c = chip_order(NZ - 1 - i)

        @pl.when(c != tp)
        def _():
            took(r3.at[c], recv=tr.at[c])

        for k in range(2):
            s = 2 * c + k

            @pl.when(s != sp)
            def _():
                rc(r3.at[c, k], r4.at[sp], us.at[0], ur.at[0], s, tp).start()

            @pl.when(s == sp)
            def _():
                r4[pl.ds(sp, 1)] = r3[c, pl.ds(k, 1)]

        return carry

    with jax.named_scope("give_back"):
        lax.fori_loop(0, NZ, give_back, 0)
    sp_wait(r4, us, ur, "w_ret")

    results = r4[...].reshape(SLOTS, COLS)
    moe = dot(q0[...], results) * w0 + dot(q1[...], results) * w1
    out[...] = kept[...] + moe

    @pl.when(sp < NSP - 1)
    def _():
        for copy in halos:
            copy.wait_send()

    with jax.named_scope("sends"):
        took(r4.at[0 : NSP - 1], send=ds_.at[0])
        took(r3.at[0 : NTP - 1], send=ts.at[0])
        for kind, ref in enumerate((v1, v1, v1, v2, v2, v2)):
            took(ref, send=ps.at[kind])
        for which in (0, 1):
            for stage in range(4):
                if which == 0 and stage == 2:
                    for q in range(4):
                        ring_sent(0, 2, q)
                else:
                    ring_sent(which, stage)


def per_device(
    stream, inner_act, gate_act, state_write, state_read, step_raw, conv_inner, conv_write,
    conv_read, step_bias, decay_log, inner_gain, out_weight, ffn_gain, expert_ids,
    expert_weights, expert_gate, expert_up, expert_down,
):
    vmem = pl.BlockSpec(memory_space=pltpu.VMEM)
    hbm = pl.BlockSpec(memory_space=pl.ANY)
    dma = pltpu.SemaphoreType.DMA
    return pl.pallas_call(
        kernel,
        name="layer",
        out_shape=jax.ShapeDtypeStruct((T, COLS), F32),
        in_specs=[vmem] * 10 + [hbm] * 9,
        out_specs=vmem,
        scratch_shapes=[
            pltpu.VMEM((T, INNER), BF16),
            pltpu.VMEM((T, INNER), BF16),
            pltpu.VMEM((T, STATE), BF16),
            pltpu.VMEM((T, STATE), BF16),
            pltpu.VMEM((INNER, D), BF16),
            pltpu.VMEM((T + 8, INNER + 2 * STATE), F32),
            pltpu.VMEM((16, INNER), BF16),
            pltpu.VMEM((16, STATE), BF16),
            pltpu.VMEM((16, STATE), BF16),
            pltpu.VMEM((2, 128), F32),
            pltpu.VMEM((NSP, 2, 128), F32),
            pltpu.VMEM((NSP, 8, 128), BF16),
            pltpu.VMEM((NSP, 8, 128), BF16),
            pltpu.VMEM((NSP, 8, 128), BF16),
            pltpu.VMEM((NSP, 8, 128), BF16),
            pltpu.VMEM((8, T), F32),
            pltpu.VMEM((T, INNER), BF16),
            pltpu.VMEM((4, 4, T, COLS), BF16),
            pltpu.VMEM((2, 2, 4, T // 4, COLS), BF16),
            pltpu.VMEM((2, 2, 4, T // 2, COLS), BF16),
            pltpu.VMEM((2, 2, 4, T // 4, COLS), BF16),
            pltpu.VMEM((2, 4, T // 2, COLS), BF16),
            pltpu.VMEM((2, 2, T // 4, COLS), BF16),
            pltpu.VMEM((2, 2, T // 2, COLS), BF16),
            pltpu.VMEM((2, 2, T // 4, COLS), BF16),
            pltpu.VMEM((T, COLS), F32),
            pltpu.VMEM((8, T), F32),
            pltpu.VMEM((NTP, 8, T), F32),
            pltpu.VMEM((T, COLS), BF16),
            pltpu.VMEM((SLOTS, T), BF16),
            pltpu.VMEM((T, SLOTS), BF16),
            pltpu.VMEM((T, SLOTS), BF16),
            pltpu.VMEM((NSP, CAP, COLS), BF16),
            pltpu.VMEM((NSP, CAP, COLS), BF16),
            pltpu.VMEM((2, CAP, D), BF16),
            pltpu.VMEM((4, 4, COLS, D), BF16),
            pltpu.VMEM((4, 4, FF, COLS), BF16),
            pltpu.VMEM((2 * CAP, FF), BF16),
            pltpu.VMEM((2, CAP, D), BF16),
            pltpu.VMEM((NTP, 2, CAP, COLS), BF16),
            pltpu.VMEM((NSP, CAP, COLS), BF16),
            dma((3,)), dma((3,)),
            dma((1,)), dma((1,)),
            dma((1,)), dma((1,)),
            dma((1,)), dma((1,)),
            dma((6,)), dma((6,)),
            dma((1,)), dma((1,)),
            dma((1,)), dma((NZ,)),
            dma((1,)), dma((1,)),
            dma((1,)), dma((NTP,)),
            dma((1,)), dma((1,)),
            dma((12,)), dma((12,)),
            dma((9,)),
        ],
        compiler_params=pltpu.CompilerParams(
            collective_id=0, has_side_effects=True, vmem_limit_bytes=60 * 1024 * 1024
        ),
    )(
        step_raw.T, step_bias.reshape(1, HEADS), decay_log.reshape(1, HEADS), conv_inner,
        conv_write.reshape(4, STATE), conv_read.reshape(4, STATE), inner_gain.reshape(1, INNER),
        ffn_gain.reshape(1, D), expert_ids.T, expert_weights.T,
        inner_act, gate_act, state_write.reshape(T, STATE), state_read.reshape(T, STATE),
        out_weight, stream, expert_gate[0].T, expert_up[0].T, expert_down[0],
    ).astype(BF16    )


def solution(mesh):
    return jax.shard_map(
        per_device,
        mesh=mesh,
        in_specs=(
            P("sp", None), P("sp", "tp"), P("sp", "tp"), P("sp", "tp", None), P("sp", "tp", None),
            P("sp", "tp"), P(None, "tp"), P(None, "tp", None), P(None, "tp", None), P("tp"),
            P("tp"), P("tp"), P("tp", None), P(), P("sp", None), P("sp", None),
            P("sp", None, "tp"), P("sp", None, "tp"), P("sp", None, "tp"),
        ),
        out_specs=P("sp", "tp"),
        check_vma=False,
    )
```

```python
import functools

import jax
import jax.numpy as jnp
from jax import lax
from jax.experimental import pallas as pl
from jax.experimental.pallas import tpu as pltpu
from jax.sharding import PartitionSpec as P

F32 = jnp.float32
BF16 = jnp.bfloat16
HIGH = lax.Precision.HIGHEST
EPS = 1e-06
NSP = 32
NZ = 16
NTP = 16
CAP = 48
T = 384
D = 2048
INNER = 256
STATE = 128
HEADS = 4
HD = 64
SLOTS = NSP * CAP
COLS = D // NTP
FF = 1024


def dot(a, b, dims=((1,), (0,)), precision=None):
    return lax.dot_general(a, b, (dims, ((), ())), precision=precision, preferred_element_type=F32)


def iota(shape, dim):
    return lax.broadcasted_iota(jnp.int32, shape, dim)


def silu(v):
    return v / (1.0 + jnp.exp(-v))


def kernel(
    raw_h, bias_h, dlog_h, tap_xh, tap_wh, tap_rh, again_h, fgain_h, ids_h, ew_h,
    inner_h, gate_h, wr_h, rd_h, ow_h, stream, wg, wu, wd,
    out,
    raw, bias, dlog, tap_x, tap_w, tap_r, again, fgain, ids, ew, inner, gate, wr, rd, ow, padf, halo_x, halo_w, halo_r, lam, rlam, spc, rs, es, re, colbuf, mixed, pbuf, v1, w1b, z1, s1, v2, w2b, z2, kept, scol,
    pm, q0, q1, sent, rx, xb, xn, gu, dn, hid, ob, r3, r4,
    hs, hr, ls, lr, as_, ar, bs, br, ps, pr, ds_, dr, fs, fr, ts, tr, us, ur, es_, er, gs, gr, loc,
):
    sp = lax.axis_index("sp")
    tp = lax.axis_index("tp")
    y = tp // 4
    x = lax.rem(tp, 4)
    z = sp // 2

    def rc(src, dst, send, recv, sp_to, tp_to):
        return pltpu.make_async_remote_copy(
            src_ref=src, dst_ref=dst, send_sem=send, recv_sem=recv,
            device_id={"sp": sp_to, "tp": tp_to}, device_id_type=pl.DeviceIdType.MESH,
        )

    def tp_of(y_, x_):
        return lax.rem(y_ + 4, 4) * 4 + lax.rem(x_ + 4, 4)

    def lanes(start, size):
        return pl.ds(pl.multiple_of(start, 128), size)

    barrier = pltpu.get_barrier_semaphore()

    def greet_sp(q, carry):
        pl.semaphore_signal(
            barrier, inc=1, device_id={"sp": lax.rem(sp + q, NSP), "tp": tp},
            device_id_type=pl.DeviceIdType.MESH,
        )
        return carry

    def greet_tp(q, carry):
        pl.semaphore_signal(
            barrier, inc=1, device_id={"sp": sp, "tp": lax.rem(tp + q, NTP)},
            device_id_type=pl.DeviceIdType.MESH,
        )
        return carry

    lax.fori_loop(1, NSP, greet_sp, 0)
    lax.fori_loop(1, NTP, greet_tp, 0)

    own = lanes(tp * COLS, COLS)
    odd = lax.rem(tp, 2)
    local = [
        pltpu.make_async_copy(wg, gu.at[y, x, pl.ds(odd * 64, 64)], loc.at[0]),
        pltpu.make_async_copy(wu, gu.at[y, x, pl.ds(64 - odd * 64, 64)], loc.at[1]),
        pltpu.make_async_copy(wd, dn.at[x], loc.at[2]),
        pltpu.make_async_copy(inner_h, inner, loc.at[3]),
        pltpu.make_async_copy(wr_h, wr, loc.at[4]),
        pltpu.make_async_copy(rd_h, rd, loc.at[5]),
        pltpu.make_async_copy(gate_h, gate, loc.at[6]),
        pltpu.make_async_copy(ow_h, ow, loc.at[7]),
        pltpu.make_async_copy(stream.at[:, own], scol, loc.at[8]),
    ]
    small = [
        pltpu.make_async_copy(src, dst, loc.at[9 + n])
        for n, (src, dst) in enumerate((
            (raw_h, raw), (bias_h, bias), (dlog_h, dlog), (tap_xh, tap_x), (tap_wh, tap_w),
            (tap_rh, tap_r), (again_h, again), (fgain_h, fgain), (ids_h, ids), (ew_h, ew),
        ))
    ]
    for copy in small + local:
        copy.start()

    with jax.named_scope("w_barrier"):
        pl.semaphore_wait(barrier, NSP - 1 + NTP - 1)

    def sp_order(i):
        step = (i + 1) // 2
        odd = lax.rem(i, 2)
        return lax.rem(sp + 16 + step * (2 * odd - 1), NSP)

    def took(ref, send=None, recv=None):
        copy = rc(ref, ref, send, recv, sp, tp) if send is not None and recv is not None else None
        if copy is None:
            sem = send if send is not None else recv
            copy = rc(ref, ref, sem, sem, sp, tp)
        if send is not None:
            copy.wait_send()
        if recv is not None:
            copy.wait_recv()

    def sp_start(src_of, dst, send, recv):
        def body(i, carry):
            e = sp_order(i)
            rc(src_of(e), dst.at[sp], send.at[0], recv.at[0], e, tp).start()
            return carry

        lax.fori_loop(0, NSP - 1, body, 0)

    def sp_wait(dst, send, recv, name):
        with jax.named_scope(name):
            took(dst.at[0 : NSP - 1], send.at[0], recv.at[0])

    def neighbour(axis, step):
        return tp_of(y, x + step) if axis == 0 else tp_of(y + step, x)

    QN = COLS // 2

    def at4(v):
        return lax.rem(v + 4, 4)

    def ring(axis, stage, quarter=None, piece=None):
        base = axis * QN
        copies = []
        for side, step in ((0, 1), (1, -1)):
            k = stage if quarter is None else 4 + quarter
            part = pl.ds(*((base + side * (QN // 2), QN // 2) if stage % 2 else (base, QN)))
            if quarter is not None:
                part = pl.ds(base + quarter * (QN // 4), QN // 4)
            back = step if stage % 2 else 0
            if stage < 2:
                to = neighbour(axis, step)
                oy, ox = (y, at4(x - back)) if axis == 0 else (at4(y - back), x)
                ref = gu.at[oy, ox, part]
            else:
                to = neighbour(1 - axis, step)
                wide = slice(None) if piece is None else pl.ds(piece * (D // 4), D // 4)
                if axis == 0:
                    ref = gu.at[at4(y - back), :, part, wide]
                else:
                    ref = gu.at[:, at4(x - back), part, wide]
            copies.append(rc(ref, ref, gs.at[k], gr.at[k], sp, to))
        return copies

    def ring_dn(stage, piece=0):
        copies = []
        for side, step in ((0, 1), (1, -1)):
            own_rows = pl.ds(piece * (FF // 2), FF // 2)
            ref = dn.at[x, own_rows] if stage == 0 else dn.at[at4(x - step), pl.ds(side * (FF // 2), FF // 2)]
            copies.append(rc(ref, ref, gs.at[8 + stage], gr.at[8 + stage], sp, tp_of(y, x + step)))
        return copies

    def rings(stage, quarter=None, piece=None):
        return [c for axis in (0, 1) for c in ring(axis, stage, quarter, piece)]

    def ring_bytes(stage, quarter=None):
        rows_ = (QN // 2 if stage % 2 else QN) if quarter is None else QN // 4
        if stage < 2:
            return gu.at[0, :, pl.ds(0, rows_)]
        return gu.at[:, :, pl.ds(0, rows_)]

    def ring_recv(stage, quarter=None):
        took(ring_bytes(stage, quarter), recv=gr.at[stage if quarter is None else 4 + quarter])

    def ring_sent(stage, quarter=None):
        took(ring_bytes(stage, quarter), send=gs.at[stage if quarter is None else 4 + quarter])

    def dn_bytes(stage):
        return dn.at[0:2] if stage == 0 else dn.at[0]

    def start(copies):
        for copy in copies:
            copy.start()

    for copy in local[:3]:
        copy.wait()
    start(rings(0))
    start(ring_dn(0, 0))

    for copy in local[3:6]:
        copy.wait()

    halos = [
        rc(ref.at[T - 16 : T], dst, hs.at[n], hr.at[n], lax.rem(sp + 1, NSP), tp)
        for n, (ref, dst) in enumerate(((inner, halo_x), (wr, halo_w), (rd, halo_r)))
    ]

    @pl.when(sp < NSP - 1)
    def _():
        for copy in halos:
            copy.start()

    for copy in small:
        copy.wait()

    rate = -jnp.exp(dlog[...])
    step = raw[...].astype(F32)
    step = jnp.concatenate([step[h : h + 1] + bias[0:1, h : h + 1] for h in range(HEADS)], axis=0)
    dtt = jnp.maximum(step, 0.0) + jnp.log1p(jnp.exp(-jnp.abs(step)))
    at = jnp.concatenate(
        [dtt[h : h + 1] * rate[0:1, h : h + 1] for h in range(HEADS)] + [jnp.zeros((4, T), F32)], axis=0
    )
    colbuf[0:4, :] = dtt
    colbuf[4:6, :] = ids[...].astype(F32)
    colbuf[6:8, :] = ew[...]
    cols = jnp.transpose(colbuf[...])
    e0, e1 = cols[:, 4:5].astype(jnp.int32), cols[:, 5:6].astype(jnp.int32)
    w0, w1 = cols[:, 6:7], cols[:, 7:8]
    head_of = iota((1, INNER), 1) >> 6

    def by_head(pick):
        v = jnp.where(head_of == 0, pick(0), pick(1))
        return jnp.where(head_of == 3, pick(3), jnp.where(head_of == 2, pick(2), v))

    dtx = by_head(lambda h: cols[:, h : h + 1])
    ratex = by_head(lambda h: rate[0:1, h : h + 1])

    lower = iota((T, T), 0) > iota((T, T), 1)
    upper = iota((T, T), 0) < iota((T, T), 1)
    ax = dtx * ratex
    cumx = dot(jnp.where(upper, 0.0, 1.0), ax, precision=HIGH)
    cumt = dot(at, jnp.where(lower, 0.0, 1.0), precision=HIGH)
    total = cumx[T - 1 : T, :]
    lam[0:1, :] = total[:, :128]
    lam[1:2, :] = total[:, 128:]

    sp_start(lambda e: lam, rlam, ls, lr)

    padf[8:, :] = jnp.concatenate([inner[...], wr[...], rd[...]], axis=1).astype(F32)

    @pl.when(sp > 0)
    def _():
        for copy in halos:
            copy.wait_recv()
        tail = jnp.concatenate([halo_x[...], halo_w[...], halo_r[...]], axis=1).astype(F32)
        padf[0:8, :] = tail[8:, :]

    @pl.when(sp == 0)
    def _():
        padf[0:8, :] = jnp.zeros((8, INNER + 2 * STATE), F32)

    taps = jnp.concatenate([tap_x[...], tap_w[...], tap_r[...]], axis=1).astype(F32)
    conv = taps[0:1, :] * padf[5 : 5 + T, :]
    for k in range(1, 4):
        conv = conv + taps[k : k + 1, :] * padf[5 + k : 5 + k + T, :]
    conv = silu(conv)
    xs = conv[:, :INNER]
    bwb = conv[:, INNER : INNER + STATE].astype(BF16)
    crb = conv[:, INNER + STATE :].astype(BF16)

    weighted = (xs * (jnp.exp(total - cumx) * dtx)).astype(BF16)
    closing = dot(bwb, weighted, ((0,), (0,))).astype(BF16)
    spc[0:16] = closing[:, :128].reshape(16, 8, 128)
    spc[16:32] = closing[:, 128:].reshape(16, 8, 128)
    sp_start(lambda e: spc.at[e], rs, as_, ar)
    rs[pl.ds(sp, 1)] = spc[pl.ds(sp, 1)]
    rlam[pl.ds(sp, 1)] = lam[...].reshape(1, 2, 128)

    xsb = xs.astype(BF16)
    rows = 128
    insides = []
    for c in range(0, T, rows):
        n = c + rows
        g = dot(crb[c:n], bwb[:n], ((1,), (1,)))
        causal = iota((rows, n), 0) + c >= iota((rows, n), 1)
        acc = jnp.zeros((rows, INNER), F32)
        for h in range(HEADS):
            diff = cumx[c:n, h * HD : h * HD + 1] - cumt[h : h + 1, :n]
            w = jnp.where(causal, jnp.exp(jnp.minimum(diff, 0.0)), 0.0) * g * dtt[h : h + 1, :n]
            xh = jnp.where(head_of == h, xsb[:n], jnp.zeros((), BF16))
            acc = acc + dot(w.astype(BF16), xh)
        insides.append(acc)
    inside = jnp.concatenate(insides, axis=0)

    with jax.named_scope("w_first_gu"):
        ring_recv(0)
    start(rings(1))
    start(ring_dn(0, 1))

    lane_e = iota((T, 128), 1)
    oh0, oh1 = lane_e == e0, lane_e == e1
    both = jnp.where(oh0 | oh1, 1.0, 0.0).astype(BF16)
    count = dot(jnp.where(lower, 1.0, 0.0).astype(BF16), both)
    t0 = e0 * CAP + jnp.sum(jnp.where(oh0, count, 0.0), axis=1, keepdims=True).astype(jnp.int32)
    t1 = e1 * CAP + jnp.sum(jnp.where(oh1, count, 0.0), axis=1, keepdims=True).astype(jnp.int32)
    for c in range(0, SLOTS, 256):
        lane = iota((T, 256), 1) + c
        q0[:, c : c + 256] = jnp.where(lane == t0, 1.0, 0.0).astype(BF16)
        q1[:, c : c + 256] = jnp.where(lane == t1, 1.0, 0.0).astype(BF16)
    e0t, e1t = ids[0:1, :], ids[1:2, :]
    sub_e = iota((NSP, T), 0)
    oh0t, oh1t = sub_e == e0t, sub_e == e1t
    botht = jnp.where(oh0t | oh1t, 1.0, 0.0).astype(BF16)
    countt = dot(botht, jnp.where(upper, 1.0, 0.0).astype(BF16))
    t0t = e0t * CAP + jnp.sum(jnp.where(oh0t, countt, 0.0), axis=0, keepdims=True).astype(jnp.int32)
    t1t = e1t * CAP + jnp.sum(jnp.where(oh1t, countt, 0.0), axis=0, keepdims=True).astype(jnp.int32)
    for c in range(0, SLOTS, 256):
        row = iota((256, T), 0) + c
        pm[c : c + 256, :] = jnp.where((row == t0t) | (row == t1t), 1.0, 0.0).astype(BF16)

    sp_wait(rlam, ls, lr, "w_lam")
    sp_wait(rs, as_, ar, "w_state1")
    half = sp // 16

    def scan(p, carry):
        es[pl.ds(p, 1)] = carry.astype(BF16).reshape(1, 8, 128)
        decay = jnp.exp(rlam[p, pl.ds(half, 1), :])
        return carry * decay + rs[p].astype(F32)

    with jax.named_scope("scan"):
        lax.fori_loop(0, NSP, scan, jnp.zeros((8, 128), F32))
    sp_start(lambda e: es.at[e], re, bs, br)
    with jax.named_scope("w_second_gu"):
        ring_recv(1)
    start(rings(2, 0))
    start(rings(2, 1, 0))
    re[pl.ds(sp, 1)] = es[pl.ds(sp, 1)]
    for copy in local[6:]:
        copy.wait()
    gact = silu(gate[...].astype(F32))
    grow = jnp.exp(cumx)
    sp_wait(re, bs, br, "w_state2")
    entering = jnp.concatenate(
        [re[0:16].astype(F32).reshape(128, 128), re[16:32].astype(F32).reshape(128, 128)], axis=1
    ).astype(BF16)
    gated = (inside + dot(crb, entering) * grow) * gact
    same = jnp.where((iota((INNER, INNER), 0) >> 6) == (iota((INNER, INNER), 1) >> 6), 1.0, 0.0)
    square = dot(gated * gated, same, precision=HIGH) * (1.0 / HD)
    mixed[...] = (gated * lax.rsqrt(square + EPS) * again[...]).astype(BF16)

    for i in range(0, NTP, 2):
        term = dot(mixed[...], ow[:, i * COLS : (i + 2) * COLS]).astype(BF16)
        pbuf[i // 4, i % 4] = term[:, :COLS]
        pbuf[i // 4, i % 4 + 1] = term[:, COLS:]

    HALF = T // 2
    PART = T // 4

    def place(h):
        return (x, y) if h == 0 else (y, x)

    def slab(h, pos, first, rows):
        if h == 0:
            return pbuf.at[:, at4(pos), pl.ds(h * HALF + first, rows)]
        return pbuf.at[at4(pos), :, pl.ds(h * HALF + first, rows)]

    def read(h, pos, first, rows):
        if h == 0:
            v = pbuf[:, pl.ds(at4(pos), 1), h * HALF + first : h * HALF + first + rows]
        else:
            v = pbuf[pl.ds(at4(pos), 1), :, h * HALF + first : h * HALF + first + rows]
        return v.reshape(4, rows, COLS).astype(F32)

    hops = [(h, side, step) for h in (0, 1) for side, step in ((0, 1), (1, -1))]

    def hop(kind, h, side, step, src, dst):
        axis = h if kind < 3 else 1 - h
        late = kind // 3
        k = late * 3 + (0 if kind % 3 == 0 else 1 + h)
        return rc(src, dst, ps.at[kind], pr.at[k], sp, neighbour(axis, step))

    relay1, own1, sum1, relay2, own2, sum2 = [], [], [], [], [], []
    for h, side, step in hops:
        p, _ = place(h)
        relay1.append(hop(0, h, side, step, slab(h, p + 2, side * PART, PART), v1.at[h, side]))
        part = pl.ds((1 - side) * PART, PART)
        own1.append(hop(1, h, side, step, slab(h, p + step, (1 - side) * PART, PART), w1b.at[h, side, :, part]))
        part = pl.ds(side * PART, PART)
        sum1.append(hop(2, h, side, step, z1.at[h, side], w1b.at[h, side, :, part]))
    start(relay1)
    start(own1)
    with jax.named_scope("w_relay1"):
        took(v1, recv=pr.at[0])
    for n, (h, side, step) in enumerate(hops):
        p, _ = place(h)
        z1[h, side] = (read(h, p + step, side * PART, PART) + v1[h, side].astype(F32)).astype(BF16)
        sum1[n].start()
    start(rings(2, 1, 1))
    for h in (0, 1):
        p, p2 = place(h)
        with jax.named_scope("w_sum1"):
            took(w1b.at[h], recv=pr.at[1 + h])
        sums4 = read(h, p, 0, HALF) + w1b[h, 0].astype(F32) + w1b[h, 1].astype(F32)
        s1[h] = sums4.astype(BF16)
        for side, step in ((0, 1), (1, -1)):
            first_, other = pl.ds(side * PART, PART), pl.ds((1 - side) * PART, PART)
            relay2.append(hop(3, h, side, step, s1.at[h, at4(p2 + 2), first_], v2.at[h, side]))
            own2.append(hop(4, h, side, step, s1.at[h, at4(p2 + step), other], w2b.at[h, side, other]))
            sum2.append(hop(5, h, side, step, z2.at[h, side], w2b.at[h, side, first_]))
        start(relay2[2 * h : 2 * h + 2])
        start(own2[2 * h : 2 * h + 2])
    start(rings(2, 1, 2))
    with jax.named_scope("w_relay2"):
        took(v2, recv=pr.at[3])
    for n, (h, side, step) in enumerate(hops):
        _, p2 = place(h)
        here = s1[h, pl.ds(at4(p2 + step), 1), side * PART : (side + 1) * PART].reshape(PART, COLS)
        z2[h, side] = (here.astype(F32) + v2[h, side].astype(F32)).astype(BF16)
        sum2[n].start()
    start(rings(2, 1, 3))
    start(rings(2, 2))
    start(rings(2, 3))
    took(dn_bytes(0), recv=gr.at[8])
    start(ring_dn(1))
    halves = []
    for h in (0, 1):
        p, p2 = place(h)
        with jax.named_scope("w_sum2"):
            took(w2b.at[h], recv=pr.at[4 + h])
        mine = pbuf[pl.ds(y, 1), pl.ds(x, 1), h * HALF : (h + 1) * HALF].reshape(HALF, COLS).astype(F32)
        for side in (0, 1):
            mine = mine + w1b[h, side, pl.ds(p2, 1)].reshape(HALF, COLS).astype(F32)
        halves.append(mine + w2b[h, 0].astype(F32) + w2b[h, 1].astype(F32))
    middle = scol[...].astype(F32) + jnp.concatenate(halves, axis=0)
    kept[...] = middle

    rows16 = middle.astype(BF16)
    for e in range(0, NSP, 4):
        picked = dot(pm[e * CAP : (e + 4) * CAP, :], rows16).astype(BF16)
        sent[e : e + 4] = picked.reshape(4, CAP, COLS)

    def dispatch(i, carry):
        e = sp_order(i)
        rc(sent.at[e], rx.at[sp], ds_.at[0], dr.at[z], e, tp).start()
        return carry

    lax.fori_loop(0, NSP - 1, dispatch, 0)
    rx[pl.ds(sp, 1)] = sent[pl.ds(sp, 1)]

    def chip_order(i):
        step = (i + 1) // 2
        odd = lax.rem(i, 2)
        return lax.rem(z + step * (2 * odd - 1) + NZ, NZ)

    def forward(i, carry):
        c = chip_order(NZ - 1 - i)
        @pl.when(c != z)
        def _():
            took(rx.at[pl.ds(2 * c, 2)], recv=dr.at[c])

        @pl.when(c == z)
        def _():
            took(rx.at[2 * c], recv=dr.at[c])

        src = rx.at[pl.ds(2 * c, 2)]

        @pl.when(c != tp)
        def _():
            rc(src, xb.at[:, :, own], fs.at[0], fr.at[0], sp, c).start()

        @pl.when(c == tp)
        def _():
            xb[:, :, own] = rx[pl.ds(2 * c, 2)]

        return carry

    with jax.named_scope("w_third_gu"):
        for q in range(4):
            ring_recv(2, q)
    start(rings(3))
    with jax.named_scope("forward"):
        lax.fori_loop(0, NZ, forward, 0)
    with jax.named_scope("w_fwd"):
        took(r3.at[0 : NTP - 1], recv=fr.at[0])
    xf = xb[...].reshape(2 * CAP, D).astype(F32)
    mean = jnp.sum(xf * xf, axis=1, keepdims=True) * (1.0 / D)
    xn[...] = (xf * lax.rsqrt(mean + EPS) * fgain[...]).astype(BF16)
    with jax.named_scope("w_fourth_gu"):
        ring_recv(3)

    low = iota((1, 128), 1) < 64

    def expert_in(i, carry):
        q = 2 * lax.rem(i, 2)
        w = gu[i // 2, pl.ds(q, 2)].reshape(256, D)
        g = dot(xn[...], w, ((1,), (1,)))
        a, b = g[:, :128], g[:, 128:]
        even = silu(a) * pltpu.roll(a, 64, 1)
        odd = silu(b) * pltpu.roll(b, 64, 1)
        units = lanes(i * 128, 128)
        hid[y, :, units] = jnp.where(low, even, odd).astype(BF16)
        for side, step in ((0, 1), (1, -1)):
            ref = hid.at[y, :, units]
            rc(ref, ref, es_.at[side], er.at[side], sp, tp_of(y + step, x)).start()
        return carry

    with jax.named_scope("expert_in"):
        lax.fori_loop(0, NTP // 2, expert_in, 0)

    def hidden_on(side, step):
        ref = hid.at[at4(y - step), :, side * (FF // 2) : (side + 1) * (FF // 2)]
        return rc(ref, ref, es_.at[2 + side], er.at[2], sp, tp_of(y + step, x))

    def hand_over(c):
        for k in range(2):
            s = 2 * c + k

            @pl.when(s != sp)
            def _():
                rc(r3.at[c, k], r4.at[sp], us.at[0], ur.at[0], s, tp).start()

            @pl.when(s == sp)
            def _():
                r4[pl.ds(sp, 1)] = r3[c, pl.ds(k, 1)]

    def expert_out(k):
        h = hid[pl.ds(k, 1)].reshape(2 * CAP, FF)
        for n in (0, 2):
            w = jnp.concatenate([dn[n], dn[n + 1]], axis=1)
            o = dot(h, w).astype(BF16)
            for m in (0, 1):
                ob[pl.ds(k, 1), n + m] = o[:, m * COLS : (m + 1) * COLS].reshape(1, 2, CAP, COLS)
        for n in range(4):
            to = tp_of(y, jnp.int32(n))

            @pl.when(x != n)
            def _():
                rc(ob.at[k, n], r3.at[k * 4 + x], ts.at[0], tr.at[k * 4 + x], sp, to).start()

            @pl.when(x == n)
            def _():
                r3[pl.ds(k * 4 + x, 1)] = ob[pl.ds(k, 1), n]
                hand_over(k * 4 + x)

    def give_back(i, carry):
        k = i // 4
        k = k + (k // 2) * (1 - 2 * lax.rem(k, 2))
        c = at4(y + k) * 4 + at4(x + i)

        @pl.when(lax.rem(i, 4) != 0)
        def _():
            took(r3.at[c], recv=tr.at[c])
            hand_over(c)

        return carry

    with jax.named_scope("w_second_dn"):
        took(dn_bytes(1), recv=gr.at[9])
    with jax.named_scope("expert_out0"):
        expert_out(y)
    with jax.named_scope("w_hid1"):
        took(hid.at[0], recv=er.at[0])
        hidden_on(0, 1).start()
        took(hid.at[0], recv=er.at[1])
        hidden_on(1, -1).start()
    with jax.named_scope("expert_out1"):
        expert_out(at4(y + 1))
        expert_out(at4(y - 1))
    with jax.named_scope("give_back0"):
        lax.fori_loop(0, 4, give_back, 0)
    with jax.named_scope("w_hid2"):
        took(hid.at[0], recv=er.at[2])
    with jax.named_scope("expert_out2"):
        expert_out(at4(y + 2))
    with jax.named_scope("give_back"):
        lax.fori_loop(4, NZ, give_back, 0)
    sp_wait(r4, us, ur, "w_ret")

    results = r4[...].reshape(SLOTS, COLS)
    moe = dot(q0[...], results) * w0 + dot(q1[...], results) * w1
    out[...] = kept[...] + moe

    @pl.when(sp < NSP - 1)
    def _():
        for copy in halos:
            copy.wait_send()

    with jax.named_scope("sends"):
        took(r3.at[0 : NTP - 1], send=fs.at[0])
        took(r4.at[0 : NSP - 1], send=ds_.at[0])
        took(r3.at[0:12], send=ts.at[0])
        for side in (0, 1):
            took(hid.at[0], send=es_.at[side])
            took(hid.at[0, :, 0 : FF // 2], send=es_.at[2 + side])
        for kind, ref in enumerate((v1, v1, v1, v2, v2, v2)):
            took(ref, send=ps.at[kind])
        for stage in (0, 1, 3):
            ring_sent(stage)
        for q in range(4):
            ring_sent(2, q)
        took(dn_bytes(0), send=gs.at[8])
        took(dn_bytes(1), send=gs.at[9])


def per_device(
    stream, inner_act, gate_act, state_write, state_read, step_raw, conv_inner, conv_write,
    conv_read, step_bias, decay_log, inner_gain, out_weight, ffn_gain, expert_ids,
    expert_weights, expert_gate, expert_up, expert_down,
):
    vmem = pl.BlockSpec(memory_space=pltpu.VMEM)
    hbm = pl.BlockSpec(memory_space=pl.ANY)
    dma = pltpu.SemaphoreType.DMA
    return pl.pallas_call(
        kernel,
        name="layer",
        out_shape=jax.ShapeDtypeStruct((T, COLS), F32),
        in_specs=[hbm] * 19,
        out_specs=vmem,
        scratch_shapes=[
            pltpu.VMEM((HEADS, T), BF16),
            pltpu.VMEM((1, HEADS), F32),
            pltpu.VMEM((1, HEADS), F32),
            pltpu.VMEM((4, INNER), BF16),
            pltpu.VMEM((4, STATE), BF16),
            pltpu.VMEM((4, STATE), BF16),
            pltpu.VMEM((1, INNER), F32),
            pltpu.VMEM((1, D), F32),
            pltpu.VMEM((2, T), jnp.int32),
            pltpu.VMEM((2, T), F32),
            pltpu.VMEM((T, INNER), BF16),
            pltpu.VMEM((T, INNER), BF16),
            pltpu.VMEM((T, STATE), BF16),
            pltpu.VMEM((T, STATE), BF16),
            pltpu.VMEM((INNER, D), BF16),
            pltpu.VMEM((T + 8, INNER + 2 * STATE), F32),
            pltpu.VMEM((16, INNER), BF16),
            pltpu.VMEM((16, STATE), BF16),
            pltpu.VMEM((16, STATE), BF16),
            pltpu.VMEM((2, 128), F32),
            pltpu.VMEM((NSP, 2, 128), F32),
            pltpu.VMEM((NSP, 8, 128), BF16),
            pltpu.VMEM((NSP, 8, 128), BF16),
            pltpu.VMEM((NSP, 8, 128), BF16),
            pltpu.VMEM((NSP, 8, 128), BF16),
            pltpu.VMEM((8, T), F32),
            pltpu.VMEM((T, INNER), BF16),
            pltpu.VMEM((4, 4, T, COLS), BF16),
            pltpu.VMEM((2, 2, 4, T // 4, COLS), BF16),
            pltpu.VMEM((2, 2, 4, T // 2, COLS), BF16),
            pltpu.VMEM((2, 2, 4, T // 4, COLS), BF16),
            pltpu.VMEM((2, 4, T // 2, COLS), BF16),
            pltpu.VMEM((2, 2, T // 4, COLS), BF16),
            pltpu.VMEM((2, 2, T // 2, COLS), BF16),
            pltpu.VMEM((2, 2, T // 4, COLS), BF16),
            pltpu.VMEM((T, COLS), F32),
            pltpu.VMEM((T, COLS), BF16),
            pltpu.VMEM((SLOTS, T), BF16),
            pltpu.VMEM((T, SLOTS), BF16),
            pltpu.VMEM((T, SLOTS), BF16),
            pltpu.VMEM((NSP, CAP, COLS), BF16),
            pltpu.VMEM((NSP, CAP, COLS), BF16),
            pltpu.VMEM((2, CAP, D), BF16),
            pltpu.VMEM((2 * CAP, D), BF16),
            pltpu.VMEM((4, 4, COLS, D), BF16),
            pltpu.VMEM((4, FF, COLS), BF16),
            pltpu.VMEM((4, 2 * CAP, FF), BF16),
            pltpu.VMEM((4, 4, 2, CAP, COLS), BF16),
            pltpu.VMEM((NTP, 2, CAP, COLS), BF16),
            pltpu.VMEM((NSP, CAP, COLS), BF16),
            dma((3,)), dma((3,)),
            dma((1,)), dma((1,)),
            dma((1,)), dma((1,)),
            dma((1,)), dma((1,)),
            dma((6,)), dma((6,)),
            dma((1,)), dma((NZ,)),
            dma((1,)), dma((1,)),
            dma((1,)), dma((NTP,)),
            dma((1,)), dma((1,)),
            dma((4,)), dma((3,)),
            dma((10,)), dma((10,)),
            dma((19,)),
        ],
        compiler_params=pltpu.CompilerParams(
            collective_id=0, has_side_effects=True, vmem_limit_bytes=60 * 1024 * 1024
        ),
    )(
        step_raw.T, step_bias.reshape(1, HEADS), decay_log.reshape(1, HEADS), conv_inner,
        conv_write.reshape(4, STATE), conv_read.reshape(4, STATE), inner_gain.reshape(1, INNER),
        ffn_gain.reshape(1, D), expert_ids.T, expert_weights.T,
        inner_act, gate_act, state_write.reshape(T, STATE), state_read.reshape(T, STATE),
        out_weight, stream, expert_gate[0].T, expert_up[0].T, expert_down[0],
    ).astype(BF16    )


def solution(mesh):
    return jax.shard_map(
        per_device,
        mesh=mesh,
        in_specs=(
            P("sp", None), P("sp", "tp"), P("sp", "tp"), P("sp", "tp", None), P("sp", "tp", None),
            P("sp", "tp"), P(None, "tp"), P(None, "tp", None), P(None, "tp", None), P("tp"),
            P("tp"), P("tp"), P("tp", None), P(), P("sp", None), P("sp", None),
            P("sp", None, "tp"), P("sp", None, "tp"), P("sp", None, "tp"),
        ),
        out_specs=P("sp", "tp"),
        check_vma=False,
    )
```

```python
import functools

import jax
import jax.numpy as jnp
from jax import lax
from jax.experimental import pallas as pl
from jax.experimental.pallas import tpu as pltpu
from jax.sharding import PartitionSpec as P

F32 = jnp.float32
BF16 = jnp.bfloat16
HIGH = lax.Precision.HIGHEST
EPS = 1e-06
NSP = 32
NZ = 16
NTP = 16
CAP = 48
T = 384
D = 2048
INNER = 256
STATE = 128
HEADS = 4
HD = 64
SLOTS = NSP * CAP
COLS = D // NTP
FF = 1024


def dot(a, b, dims=((1,), (0,)), precision=None):
    return lax.dot_general(a, b, (dims, ((), ())), precision=precision, preferred_element_type=F32)


def iota(shape, dim):
    return lax.broadcasted_iota(jnp.int32, shape, dim)


def silu(v):
    return v / (1.0 + jnp.exp(-v))


def kernel(
    raw_h, bias_h, dlog_h, tap_xh, tap_wh, tap_rh, again_h, fgain_h, ids_h, ew_h,
    inner_h, gate_h, wr_h, rd_h, ow_h, stream, wg, wu, wd,
    out,
    raw, bias, dlog, tap_x, tap_w, tap_r, again, fgain, ids, ew, inner, gate, wr, rd, ow, padf, halo_x, halo_w, halo_r, lam, rlam, spc, rs, es, re, colbuf, mixed, pbuf, v1, w1b, z1, s1, v2, w2b, z2, kept, scol,
    pm, q0, q1, sent, rx, xb, xn, gu, dn, hid, ob, r3, r4,
    hs, hr, ls, lr, as_, ar, bs, br, ps, pr, ds_, dr, fs, fr, ts, tr, us, ur, es_, er, gs, gr, loc,
):
    sp = lax.axis_index("sp")
    tp = lax.axis_index("tp")
    y = tp // 4
    x = lax.rem(tp, 4)
    z = sp // 2

    def rc(src, dst, send, recv, sp_to, tp_to):
        return pltpu.make_async_remote_copy(
            src_ref=src, dst_ref=dst, send_sem=send, recv_sem=recv,
            device_id={"sp": sp_to, "tp": tp_to}, device_id_type=pl.DeviceIdType.MESH,
        )

    def tp_of(y_, x_):
        return lax.rem(y_ + 4, 4) * 4 + lax.rem(x_ + 4, 4)

    def lanes(start, size):
        return pl.ds(pl.multiple_of(start, 128), size)

    barrier = pltpu.get_barrier_semaphore()

    def greet_sp(q, carry):
        pl.semaphore_signal(
            barrier, inc=1, device_id={"sp": lax.rem(sp + q, NSP), "tp": tp},
            device_id_type=pl.DeviceIdType.MESH,
        )
        return carry

    def greet_tp(q, carry):
        pl.semaphore_signal(
            barrier, inc=1, device_id={"sp": sp, "tp": lax.rem(tp + q, NTP)},
            device_id_type=pl.DeviceIdType.MESH,
        )
        return carry

    lax.fori_loop(1, NSP, greet_sp, 0)
    lax.fori_loop(1, NTP, greet_tp, 0)

    own = lanes(tp * COLS, COLS)
    odd = lax.rem(tp, 2)
    local = [
        pltpu.make_async_copy(wg, gu.at[y, x, pl.ds(odd * 64, 64)], loc.at[0]),
        pltpu.make_async_copy(wu, gu.at[y, x, pl.ds(64 - odd * 64, 64)], loc.at[1]),
        pltpu.make_async_copy(wd, dn.at[x], loc.at[2]),
        pltpu.make_async_copy(inner_h, inner, loc.at[3]),
        pltpu.make_async_copy(wr_h, wr, loc.at[4]),
        pltpu.make_async_copy(rd_h, rd, loc.at[5]),
        pltpu.make_async_copy(gate_h, gate, loc.at[6]),
        pltpu.make_async_copy(ow_h, ow, loc.at[7]),
        pltpu.make_async_copy(stream.at[:, own], scol, loc.at[8]),
    ]
    small = [
        pltpu.make_async_copy(src, dst, loc.at[9 + n])
        for n, (src, dst) in enumerate((
            (raw_h, raw), (bias_h, bias), (dlog_h, dlog), (tap_xh, tap_x), (tap_wh, tap_w),
            (tap_rh, tap_r), (again_h, again), (fgain_h, fgain), (ids_h, ids), (ew_h, ew),
        ))
    ]
    for copy in small + local:
        copy.start()

    with jax.named_scope("w_barrier"):
        pl.semaphore_wait(barrier, NSP - 1 + NTP - 1)

    def sp_order(i):
        step = (i + 1) // 2
        odd = lax.rem(i, 2)
        return lax.rem(sp + 16 + step * (2 * odd - 1), NSP)

    def took(ref, send=None, recv=None):
        copy = rc(ref, ref, send, recv, sp, tp) if send is not None and recv is not None else None
        if copy is None:
            sem = send if send is not None else recv
            copy = rc(ref, ref, sem, sem, sp, tp)
        if send is not None:
            copy.wait_send()
        if recv is not None:
            copy.wait_recv()

    def sp_start(src_of, dst, send, recv):
        def body(i, carry):
            e = sp_order(i)
            rc(src_of(e), dst.at[sp], send.at[0], recv.at[0], e, tp).start()
            return carry

        lax.fori_loop(0, NSP - 1, body, 0)

    def sp_wait(dst, send, recv, name):
        with jax.named_scope(name):
            took(dst.at[0 : NSP - 1], send.at[0], recv.at[0])

    def neighbour(axis, step):
        return tp_of(y, x + step) if axis == 0 else tp_of(y + step, x)

    WIDE = ((0, 1152), (1152, 896))
    PIECES = (((0, 384), (384, 384), (768, 384)), ((1152, 256), (1408, 256), (1664, 384)))

    def at4(v):
        return lax.rem(v + 4, 4)

    def ring(axis, stage, quarter=None, piece=None):
        wide = pl.ds(*(WIDE[axis] if piece is None else PIECES[axis][piece]))
        copies = []
        for side, step in ((0, 1), (1, -1)):
            k = stage if quarter is None else 4 + quarter
            part = pl.ds(side * (COLS // 2), COLS // 2) if stage % 2 else pl.ds(0, COLS)
            if quarter is not None:
                part = pl.ds(quarter * (COLS // 4), COLS // 4)
            back = step if stage % 2 else 0
            if stage < 2:
                to = neighbour(axis, step)
                oy, ox = (y, at4(x - back)) if axis == 0 else (at4(y - back), x)
                ref = gu.at[oy, ox, part, wide]
            else:
                to = neighbour(1 - axis, step)
                if axis == 0:
                    ref = gu.at[at4(y - back), :, part, wide]
                else:
                    ref = gu.at[:, at4(x - back), part, wide]
            copies.append(rc(ref, ref, gs.at[k], gr.at[k], sp, to))
        return copies

    def ring_dn(stage, piece=0):
        copies = []
        for side, step in ((0, 1), (1, -1)):
            own_rows = pl.ds(piece * (FF // 2), FF // 2)
            ref = dn.at[x, own_rows] if stage == 0 else dn.at[at4(x - step), pl.ds(side * (FF // 2), FF // 2)]
            copies.append(rc(ref, ref, gs.at[8 + stage], gr.at[8 + stage], sp, tp_of(y, x + step)))
        return copies

    def rings(stage, quarter=None, piece=None):
        return [c for axis in (0, 1) for c in ring(axis, stage, quarter, piece)]

    def ring_bytes(stage, quarter=None):
        if stage < 2:
            return gu.at[0, 0 : 2 - stage]
        rows_ = COLS // 2 if quarter is None else COLS // 4
        return gu.at[0:2, :, pl.ds(0, rows_)]

    def ring_recv(stage, quarter=None):
        took(ring_bytes(stage, quarter), recv=gr.at[stage if quarter is None else 4 + quarter])

    def ring_sent(stage, quarter=None):
        took(ring_bytes(stage, quarter), send=gs.at[stage if quarter is None else 4 + quarter])

    def dn_bytes(stage):
        return dn.at[0:2] if stage == 0 else dn.at[0]

    def start(copies):
        for copy in copies:
            copy.start()

    for copy in local[:3]:
        copy.wait()
    start(rings(0))
    start(ring_dn(0, 0))

    for copy in local[3:6]:
        copy.wait()

    halos = [
        rc(ref.at[T - 16 : T], dst, hs.at[n], hr.at[n], lax.rem(sp + 1, NSP), tp)
        for n, (ref, dst) in enumerate(((inner, halo_x), (wr, halo_w), (rd, halo_r)))
    ]

    @pl.when(sp < NSP - 1)
    def _():
        for copy in halos:
            copy.start()

    for copy in small:
        copy.wait()

    rate = -jnp.exp(dlog[...])
    step = raw[...].astype(F32)
    step = jnp.concatenate([step[h : h + 1] + bias[0:1, h : h + 1] for h in range(HEADS)], axis=0)
    dtt = jnp.maximum(step, 0.0) + jnp.log1p(jnp.exp(-jnp.abs(step)))
    at = jnp.concatenate(
        [dtt[h : h + 1] * rate[0:1, h : h + 1] for h in range(HEADS)] + [jnp.zeros((4, T), F32)], axis=0
    )
    colbuf[0:4, :] = dtt
    colbuf[4:6, :] = ids[...].astype(F32)
    colbuf[6:8, :] = ew[...]
    cols = jnp.transpose(colbuf[...])
    e0, e1 = cols[:, 4:5].astype(jnp.int32), cols[:, 5:6].astype(jnp.int32)
    w0, w1 = cols[:, 6:7], cols[:, 7:8]
    head_of = iota((1, INNER), 1) >> 6

    def by_head(pick):
        v = jnp.where(head_of == 0, pick(0), pick(1))
        return jnp.where(head_of == 3, pick(3), jnp.where(head_of == 2, pick(2), v))

    dtx = by_head(lambda h: cols[:, h : h + 1])
    ratex = by_head(lambda h: rate[0:1, h : h + 1])

    lower = iota((T, T), 0) > iota((T, T), 1)
    upper = iota((T, T), 0) < iota((T, T), 1)
    ax = dtx * ratex
    cumx = dot(jnp.where(upper, 0.0, 1.0), ax, precision=HIGH)
    cumt = dot(at, jnp.where(lower, 0.0, 1.0), precision=HIGH)
    total = cumx[T - 1 : T, :]
    lam[0:1, :] = total[:, :128]
    lam[1:2, :] = total[:, 128:]

    sp_start(lambda e: lam, rlam, ls, lr)

    padf[8:, :] = jnp.concatenate([inner[...], wr[...], rd[...]], axis=1).astype(F32)

    @pl.when(sp > 0)
    def _():
        for copy in halos:
            copy.wait_recv()
        tail = jnp.concatenate([halo_x[...], halo_w[...], halo_r[...]], axis=1).astype(F32)
        padf[0:8, :] = tail[8:, :]

    @pl.when(sp == 0)
    def _():
        padf[0:8, :] = jnp.zeros((8, INNER + 2 * STATE), F32)

    taps = jnp.concatenate([tap_x[...], tap_w[...], tap_r[...]], axis=1).astype(F32)
    conv = taps[0:1, :] * padf[5 : 5 + T, :]
    for k in range(1, 4):
        conv = conv + taps[k : k + 1, :] * padf[5 + k : 5 + k + T, :]
    conv = silu(conv)
    xs = conv[:, :INNER]
    bwb = conv[:, INNER : INNER + STATE].astype(BF16)
    crb = conv[:, INNER + STATE :].astype(BF16)

    weighted = (xs * (jnp.exp(total - cumx) * dtx)).astype(BF16)
    closing = dot(bwb, weighted, ((0,), (0,))).astype(BF16)
    spc[0:16] = closing[:, :128].reshape(16, 8, 128)
    spc[16:32] = closing[:, 128:].reshape(16, 8, 128)
    sp_start(lambda e: spc.at[e], rs, as_, ar)
    rs[pl.ds(sp, 1)] = spc[pl.ds(sp, 1)]
    rlam[pl.ds(sp, 1)] = lam[...].reshape(1, 2, 128)

    xsb = xs.astype(BF16)
    rows = 128
    insides = []
    for c in range(0, T, rows):
        n = c + rows
        g = dot(crb[c:n], bwb[:n], ((1,), (1,)))
        causal = iota((rows, n), 0) + c >= iota((rows, n), 1)
        acc = jnp.zeros((rows, INNER), F32)
        for h in range(HEADS):
            diff = cumx[c:n, h * HD : h * HD + 1] - cumt[h : h + 1, :n]
            w = jnp.where(causal, jnp.exp(jnp.minimum(diff, 0.0)), 0.0) * g * dtt[h : h + 1, :n]
            xh = jnp.where(head_of == h, xsb[:n], jnp.zeros((), BF16))
            acc = acc + dot(w.astype(BF16), xh)
        insides.append(acc)
    inside = jnp.concatenate(insides, axis=0)

    with jax.named_scope("w_first_gu"):
        ring_recv(0)
    start(rings(1))
    start(ring_dn(0, 1))

    lane_e = iota((T, 128), 1)
    oh0, oh1 = lane_e == e0, lane_e == e1
    both = jnp.where(oh0 | oh1, 1.0, 0.0).astype(BF16)
    count = dot(jnp.where(lower, 1.0, 0.0).astype(BF16), both)
    t0 = e0 * CAP + jnp.sum(jnp.where(oh0, count, 0.0), axis=1, keepdims=True).astype(jnp.int32)
    t1 = e1 * CAP + jnp.sum(jnp.where(oh1, count, 0.0), axis=1, keepdims=True).astype(jnp.int32)
    for c in range(0, SLOTS, 256):
        lane = iota((T, 256), 1) + c
        q0[:, c : c + 256] = jnp.where(lane == t0, 1.0, 0.0).astype(BF16)
        q1[:, c : c + 256] = jnp.where(lane == t1, 1.0, 0.0).astype(BF16)
    e0t, e1t = ids[0:1, :], ids[1:2, :]
    sub_e = iota((NSP, T), 0)
    oh0t, oh1t = sub_e == e0t, sub_e == e1t
    botht = jnp.where(oh0t | oh1t, 1.0, 0.0).astype(BF16)
    countt = dot(botht, jnp.where(upper, 1.0, 0.0).astype(BF16))
    t0t = e0t * CAP + jnp.sum(jnp.where(oh0t, countt, 0.0), axis=0, keepdims=True).astype(jnp.int32)
    t1t = e1t * CAP + jnp.sum(jnp.where(oh1t, countt, 0.0), axis=0, keepdims=True).astype(jnp.int32)
    for c in range(0, SLOTS, 256):
        row = iota((256, T), 0) + c
        pm[c : c + 256, :] = jnp.where((row == t0t) | (row == t1t), 1.0, 0.0).astype(BF16)

    sp_wait(rlam, ls, lr, "w_lam")
    sp_wait(rs, as_, ar, "w_state1")
    half = sp // 16

    def scan(p, carry):
        es[pl.ds(p, 1)] = carry.astype(BF16).reshape(1, 8, 128)
        decay = jnp.exp(rlam[p, pl.ds(half, 1), :])
        return carry * decay + rs[p].astype(F32)

    with jax.named_scope("scan"):
        lax.fori_loop(0, NSP, scan, jnp.zeros((8, 128), F32))
    sp_start(lambda e: es.at[e], re, bs, br)
    with jax.named_scope("w_second_gu"):
        ring_recv(1)
    start(rings(2, 0))
    start(rings(2, 1, 0))
    re[pl.ds(sp, 1)] = es[pl.ds(sp, 1)]
    for copy in local[6:]:
        copy.wait()
    gact = silu(gate[...].astype(F32))
    grow = jnp.exp(cumx)
    sp_wait(re, bs, br, "w_state2")
    entering = jnp.concatenate(
        [re[0:16].astype(F32).reshape(128, 128), re[16:32].astype(F32).reshape(128, 128)], axis=1
    ).astype(BF16)
    gated = (inside + dot(crb, entering) * grow) * gact
    same = jnp.where((iota((INNER, INNER), 0) >> 6) == (iota((INNER, INNER), 1) >> 6), 1.0, 0.0)
    square = dot(gated * gated, same, precision=HIGH) * (1.0 / HD)
    mixed[...] = (gated * lax.rsqrt(square + EPS) * again[...]).astype(BF16)

    for i in range(0, NTP, 2):
        term = dot(mixed[...], ow[:, i * COLS : (i + 2) * COLS]).astype(BF16)
        pbuf[i // 4, i % 4] = term[:, :COLS]
        pbuf[i // 4, i % 4 + 1] = term[:, COLS:]

    HALF = T // 2
    PART = T // 4

    def place(h):
        return (x, y) if h == 0 else (y, x)

    def slab(h, pos, first, rows):
        if h == 0:
            return pbuf.at[:, at4(pos), pl.ds(h * HALF + first, rows)]
        return pbuf.at[at4(pos), :, pl.ds(h * HALF + first, rows)]

    def read(h, pos, first, rows):
        if h == 0:
            v = pbuf[:, pl.ds(at4(pos), 1), h * HALF + first : h * HALF + first + rows]
        else:
            v = pbuf[pl.ds(at4(pos), 1), :, h * HALF + first : h * HALF + first + rows]
        return v.reshape(4, rows, COLS).astype(F32)

    hops = [(h, side, step) for h in (0, 1) for side, step in ((0, 1), (1, -1))]

    def hop(kind, h, side, step, src, dst):
        axis = h if kind < 3 else 1 - h
        late = kind // 3
        k = late * 3 + (0 if kind % 3 == 0 else 1 + h)
        return rc(src, dst, ps.at[kind], pr.at[k], sp, neighbour(axis, step))

    relay1, own1, sum1, relay2, own2, sum2 = [], [], [], [], [], []
    for h, side, step in hops:
        p, _ = place(h)
        relay1.append(hop(0, h, side, step, slab(h, p + 2, side * PART, PART), v1.at[h, side]))
        part = pl.ds((1 - side) * PART, PART)
        own1.append(hop(1, h, side, step, slab(h, p + step, (1 - side) * PART, PART), w1b.at[h, side, :, part]))
        part = pl.ds(side * PART, PART)
        sum1.append(hop(2, h, side, step, z1.at[h, side], w1b.at[h, side, :, part]))
    start(relay1)
    start(own1)
    with jax.named_scope("w_relay1"):
        took(v1, recv=pr.at[0])
    for n, (h, side, step) in enumerate(hops):
        p, _ = place(h)
        z1[h, side] = (read(h, p + step, side * PART, PART) + v1[h, side].astype(F32)).astype(BF16)
        sum1[n].start()
    start(rings(2, 1, 1))
    for h in (0, 1):
        p, p2 = place(h)
        with jax.named_scope("w_sum1"):
            took(w1b.at[h], recv=pr.at[1 + h])
        sums4 = read(h, p, 0, HALF) + w1b[h, 0].astype(F32) + w1b[h, 1].astype(F32)
        s1[h] = sums4.astype(BF16)
        for side, step in ((0, 1), (1, -1)):
            first_, other = pl.ds(side * PART, PART), pl.ds((1 - side) * PART, PART)
            relay2.append(hop(3, h, side, step, s1.at[h, at4(p2 + 2), first_], v2.at[h, side]))
            own2.append(hop(4, h, side, step, s1.at[h, at4(p2 + step), other], w2b.at[h, side, other]))
            sum2.append(hop(5, h, side, step, z2.at[h, side], w2b.at[h, side, first_]))
        start(relay2[2 * h : 2 * h + 2])
        start(own2[2 * h : 2 * h + 2])
    start(rings(2, 1, 2))
    with jax.named_scope("w_relay2"):
        took(v2, recv=pr.at[3])
    for n, (h, side, step) in enumerate(hops):
        _, p2 = place(h)
        here = s1[h, pl.ds(at4(p2 + step), 1), side * PART : (side + 1) * PART].reshape(PART, COLS)
        z2[h, side] = (here.astype(F32) + v2[h, side].astype(F32)).astype(BF16)
        sum2[n].start()
    start(rings(2, 2))
    start(rings(2, 3))
    halves = []
    for h in (0, 1):
        p, p2 = place(h)
        with jax.named_scope("w_sum2"):
            took(w2b.at[h], recv=pr.at[4 + h])
        mine = pbuf[pl.ds(y, 1), pl.ds(x, 1), h * HALF : (h + 1) * HALF].reshape(HALF, COLS).astype(F32)
        for side in (0, 1):
            mine = mine + w1b[h, side, pl.ds(p2, 1)].reshape(HALF, COLS).astype(F32)
        halves.append(mine + w2b[h, 0].astype(F32) + w2b[h, 1].astype(F32))
    middle = scol[...].astype(F32) + jnp.concatenate(halves, axis=0)
    kept[...] = middle

    rows16 = middle.astype(BF16)
    for e in range(0, NSP, 4):
        picked = dot(pm[e * CAP : (e + 4) * CAP, :], rows16).astype(BF16)
        sent[e : e + 4] = picked.reshape(4, CAP, COLS)

    def dispatch(i, carry):
        e = sp_order(i)
        rc(sent.at[e], rx.at[sp], ds_.at[0], dr.at[z], e, tp).start()
        return carry

    lax.fori_loop(0, NSP - 1, dispatch, 0)
    rx[pl.ds(sp, 1)] = sent[pl.ds(sp, 1)]

    def chip_order(i):
        step = (i + 1) // 2
        odd = lax.rem(i, 2)
        return lax.rem(z + step * (2 * odd - 1) + NZ, NZ)

    def forward(i, carry):
        c = chip_order(NZ - 1 - i)
        @pl.when(c != z)
        def _():
            took(rx.at[pl.ds(2 * c, 2)], recv=dr.at[c])

        @pl.when(c == z)
        def _():
            took(rx.at[2 * c], recv=dr.at[c])

        src = rx.at[pl.ds(2 * c, 2)]

        @pl.when(c != tp)
        def _():
            rc(src, xb.at[:, :, own], fs.at[0], fr.at[0], sp, c).start()

        @pl.when(c == tp)
        def _():
            xb[:, :, own] = rx[pl.ds(2 * c, 2)]

        return carry

    with jax.named_scope("w_third_gu"):
        for q in range(4):
            ring_recv(2, q)
    start(rings(3))
    with jax.named_scope("forward"):
        lax.fori_loop(0, NZ, forward, 0)
    took(dn_bytes(0), recv=gr.at[8])
    start(ring_dn(1))
    with jax.named_scope("w_fwd"):
        took(r3.at[0 : NTP - 1], recv=fr.at[0])
    xf = xb[...].reshape(2 * CAP, D).astype(F32)
    mean = jnp.sum(xf * xf, axis=1, keepdims=True) * (1.0 / D)
    xn[...] = (xf * lax.rsqrt(mean + EPS) * fgain[...]).astype(BF16)
    with jax.named_scope("w_fourth_gu"):
        ring_recv(3)

    low = iota((1, 128), 1) < 64

    def expert_in(i, carry):
        q = 2 * lax.rem(i, 2)
        w = gu[i // 2, pl.ds(q, 2)].reshape(256, D)
        g = dot(xn[...], w, ((1,), (1,)))
        a, b = g[:, :128], g[:, 128:]
        even = silu(a) * pltpu.roll(a, 64, 1)
        odd = silu(b) * pltpu.roll(b, 64, 1)
        units = lanes(i * 128, 128)
        hid[y, :, units] = jnp.where(low, even, odd).astype(BF16)
        for side, step in ((0, 1), (1, -1)):
            ref = hid.at[y, :, units]
            rc(ref, ref, es_.at[side], er.at[side], sp, tp_of(y + step, x)).start()
        return carry

    with jax.named_scope("expert_in"):
        lax.fori_loop(0, NTP // 2, expert_in, 0)

    def hidden_on(side, step):
        ref = hid.at[at4(y - step), :, side * (FF // 2) : (side + 1) * (FF // 2)]
        return rc(ref, ref, es_.at[2 + side], er.at[2], sp, tp_of(y + step, x))

    def hand_over(c):
        for k in range(2):
            s = 2 * c + k

            @pl.when(s != sp)
            def _():
                rc(r3.at[c, k], r4.at[sp], us.at[0], ur.at[0], s, tp).start()

            @pl.when(s == sp)
            def _():
                r4[pl.ds(sp, 1)] = r3[c, pl.ds(k, 1)]

    def expert_out(k):
        h = hid[pl.ds(k, 1)].reshape(2 * CAP, FF)
        for n in (0, 2):
            w = jnp.concatenate([dn[n], dn[n + 1]], axis=1)
            o = dot(h, w).astype(BF16)
            for m in (0, 1):
                ob[pl.ds(k, 1), n + m] = o[:, m * COLS : (m + 1) * COLS].reshape(1, 2, CAP, COLS)
        for n in range(4):
            to = tp_of(y, jnp.int32(n))

            @pl.when(x != n)
            def _():
                rc(ob.at[k, n], r3.at[k * 4 + x], ts.at[0], tr.at[k * 4 + x], sp, to).start()

            @pl.when(x == n)
            def _():
                r3[pl.ds(k * 4 + x, 1)] = ob[pl.ds(k, 1), n]
                hand_over(k * 4 + x)

    def give_back(i, carry):
        k = i // 4
        k = k + (k // 2) * (1 - 2 * lax.rem(k, 2))
        c = at4(y + k) * 4 + at4(x + i)

        @pl.when(lax.rem(i, 4) != 0)
        def _():
            took(r3.at[c], recv=tr.at[c])
            hand_over(c)

        return carry

    with jax.named_scope("w_second_dn"):
        took(dn_bytes(1), recv=gr.at[9])
    with jax.named_scope("expert_out0"):
        expert_out(y)
    with jax.named_scope("w_hid1"):
        took(hid.at[0], recv=er.at[0])
        hidden_on(0, 1).start()
        took(hid.at[0], recv=er.at[1])
        hidden_on(1, -1).start()
    with jax.named_scope("expert_out1"):
        expert_out(at4(y + 1))
        expert_out(at4(y - 1))
    with jax.named_scope("give_back0"):
        lax.fori_loop(0, 4, give_back, 0)
    with jax.named_scope("w_hid2"):
        took(hid.at[0], recv=er.at[2])
    with jax.named_scope("expert_out2"):
        expert_out(at4(y + 2))
    with jax.named_scope("give_back"):
        lax.fori_loop(4, NZ, give_back, 0)
    sp_wait(r4, us, ur, "w_ret")

    results = r4[...].reshape(SLOTS, COLS)
    moe = dot(q0[...], results) * w0 + dot(q1[...], results) * w1
    out[...] = kept[...] + moe

    @pl.when(sp < NSP - 1)
    def _():
        for copy in halos:
            copy.wait_send()

    with jax.named_scope("sends"):
        took(r3.at[0 : NTP - 1], send=fs.at[0])
        took(r4.at[0 : NSP - 1], send=ds_.at[0])
        took(r3.at[0:12], send=ts.at[0])
        for side in (0, 1):
            took(hid.at[0], send=es_.at[side])
            took(hid.at[0, :, 0 : FF // 2], send=es_.at[2 + side])
        for kind, ref in enumerate((v1, v1, v1, v2, v2, v2)):
            took(ref, send=ps.at[kind])
        for stage in (0, 1, 3):
            ring_sent(stage)
        for q in range(4):
            ring_sent(2, q)
        took(dn_bytes(0), send=gs.at[8])
        took(dn_bytes(1), send=gs.at[9])


def per_device(
    stream, inner_act, gate_act, state_write, state_read, step_raw, conv_inner, conv_write,
    conv_read, step_bias, decay_log, inner_gain, out_weight, ffn_gain, expert_ids,
    expert_weights, expert_gate, expert_up, expert_down,
):
    vmem = pl.BlockSpec(memory_space=pltpu.VMEM)
    hbm = pl.BlockSpec(memory_space=pl.ANY)
    dma = pltpu.SemaphoreType.DMA
    return pl.pallas_call(
        kernel,
        name="layer",
        out_shape=jax.ShapeDtypeStruct((T, COLS), F32),
        in_specs=[hbm] * 19,
        out_specs=vmem,
        scratch_shapes=[
            pltpu.VMEM((HEADS, T), BF16),
            pltpu.VMEM((1, HEADS), F32),
            pltpu.VMEM((1, HEADS), F32),
            pltpu.VMEM((4, INNER), BF16),
            pltpu.VMEM((4, STATE), BF16),
            pltpu.VMEM((4, STATE), BF16),
            pltpu.VMEM((1, INNER), F32),
            pltpu.VMEM((1, D), F32),
            pltpu.VMEM((2, T), jnp.int32),
            pltpu.VMEM((2, T), F32),
            pltpu.VMEM((T, INNER), BF16),
            pltpu.VMEM((T, INNER), BF16),
            pltpu.VMEM((T, STATE), BF16),
            pltpu.VMEM((T, STATE), BF16),
            pltpu.VMEM((INNER, D), BF16),
            pltpu.VMEM((T + 8, INNER + 2 * STATE), F32),
            pltpu.VMEM((16, INNER), BF16),
            pltpu.VMEM((16, STATE), BF16),
            pltpu.VMEM((16, STATE), BF16),
            pltpu.VMEM((2, 128), F32),
            pltpu.VMEM((NSP, 2, 128), F32),
            pltpu.VMEM((NSP, 8, 128), BF16),
            pltpu.VMEM((NSP, 8, 128), BF16),
            pltpu.VMEM((NSP, 8, 128), BF16),
            pltpu.VMEM((NSP, 8, 128), BF16),
            pltpu.VMEM((8, T), F32),
            pltpu.VMEM((T, INNER), BF16),
            pltpu.VMEM((4, 4, T, COLS), BF16),
            pltpu.VMEM((2, 2, 4, T // 4, COLS), BF16),
            pltpu.VMEM((2, 2, 4, T // 2, COLS), BF16),
            pltpu.VMEM((2, 2, 4, T // 4, COLS), BF16),
            pltpu.VMEM((2, 4, T // 2, COLS), BF16),
            pltpu.VMEM((2, 2, T // 4, COLS), BF16),
            pltpu.VMEM((2, 2, T // 2, COLS), BF16),
            pltpu.VMEM((2, 2, T // 4, COLS), BF16),
            pltpu.VMEM((T, COLS), F32),
            pltpu.VMEM((T, COLS), BF16),
            pltpu.VMEM((SLOTS, T), BF16),
            pltpu.VMEM((T, SLOTS), BF16),
            pltpu.VMEM((T, SLOTS), BF16),
            pltpu.VMEM((NSP, CAP, COLS), BF16),
            pltpu.VMEM((NSP, CAP, COLS), BF16),
            pltpu.VMEM((2, CAP, D), BF16),
            pltpu.VMEM((2 * CAP, D), BF16),
            pltpu.VMEM((4, 4, COLS, D), BF16),
            pltpu.VMEM((4, FF, COLS), BF16),
            pltpu.VMEM((4, 2 * CAP, FF), BF16),
            pltpu.VMEM((4, 4, 2, CAP, COLS), BF16),
            pltpu.VMEM((NTP, 2, CAP, COLS), BF16),
            pltpu.VMEM((NSP, CAP, COLS), BF16),
            dma((3,)), dma((3,)),
            dma((1,)), dma((1,)),
            dma((1,)), dma((1,)),
            dma((1,)), dma((1,)),
            dma((6,)), dma((6,)),
            dma((1,)), dma((NZ,)),
            dma((1,)), dma((1,)),
            dma((1,)), dma((NTP,)),
            dma((1,)), dma((1,)),
            dma((4,)), dma((3,)),
            dma((10,)), dma((10,)),
            dma((19,)),
        ],
        compiler_params=pltpu.CompilerParams(
            collective_id=0, has_side_effects=True, vmem_limit_bytes=60 * 1024 * 1024
        ),
    )(
        step_raw.T, step_bias.reshape(1, HEADS), decay_log.reshape(1, HEADS), conv_inner,
        conv_write.reshape(4, STATE), conv_read.reshape(4, STATE), inner_gain.reshape(1, INNER),
        ffn_gain.reshape(1, D), expert_ids.T, expert_weights.T,
        inner_act, gate_act, state_write.reshape(T, STATE), state_read.reshape(T, STATE),
        out_weight, stream, expert_gate[0].T, expert_up[0].T, expert_down[0],
    ).astype(BF16    )


def solution(mesh):
    return jax.shard_map(
        per_device,
        mesh=mesh,
        in_specs=(
            P("sp", None), P("sp", "tp"), P("sp", "tp"), P("sp", "tp", None), P("sp", "tp", None),
            P("sp", "tp"), P(None, "tp"), P(None, "tp", None), P(None, "tp", None), P("tp"),
            P("tp"), P("tp"), P("tp", None), P(), P("sp", None), P("sp", None),
            P("sp", None, "tp"), P("sp", None, "tp"), P("sp", None, "tp"),
        ),
        out_specs=P("sp", "tp"),
        check_vma=False,
    )
```
